32 devices in a mesh: fs: 8 (over z, x), tp: 4 (over y, core).
Axes of the slice: x: 2, y: 2, z: 4, core: 2. Of those that a mesh axis runs over, the one named last changes fastest.
Arguments:
- inputs: bfloat16 [8192, 4096], P('fs'), may hold values from -8 to 8
- value_cot: bfloat16 [8192, 2048], P('fs', 'tp'), may hold values from -0.015625 to 0.015625
- gate_cot: bfloat16 [8192, 2048], P('fs', 'tp'), may hold values from -0.015625 to 0.015625
- out_cot: bfloat16 [8192, 4096], P('fs'), may hold values from -0.0234375 to 0.0234375
- conv_output: bfloat16 [8192, 2048], P('fs', 'tp'), may hold values from -6 to 6
- factors: bfloat16 [3, 4096, 256], P(None, 'fs'), may hold values from -0.375 to 0.375
- value_weight: float32 [4096, 2048], P('fs', 'tp'), may hold values from -0.09375 to 0.09375
- gate_weight: float32 [4096, 2048], P('fs', 'tp'), may hold values from -0.09375 to 0.09375
- out_weight: float32 [2048, 4096], P('tp', 'fs'), may hold values from -0.125 to 0.125
- first_moment: float32 [3, 256, 2048], P(None, 'fs', 'tp'), may hold values from -7.2 to 7.2
- second_moment: float32 [3, 256, 2048], P(None, 'fs', 'tp'), may hold values from 0.005 to 0.05
Outputs:
- new_first: float32 [3, 256, 2048], P(None, 'fs', 'tp')
- new_second: float32 [3, 256, 2048], P(None, 'fs', 'tp')
- value_update: float32 [4096, 2048], P('fs', 'tp')
- gate_update: float32 [4096, 2048], P('fs', 'tp')
- out_update: float32 [2048, 4096], P('tp', 'fs')
- value_copy: bfloat16 [4096, 2048], P(None, 'tp')
- gate_copy: bfloat16 [4096, 2048], P(None, 'tp')
- out_copy: bfloat16 [2048, 4096], P('tp')
The draws below stay inside these ranges and needn't reach their ends.
All inputs are finite; a program needn't handle non-finite values.
Results may differ from the reference program's by a relative error of at most 0.001.
Values may be sent and summed in bfloat16 or wider, within the bound.
A program may use at most 128 MiB of HBM per device.

```python
import math
import jax
import jax.numpy as jnp
from jax import lax

D = 4096
C = 2048
RANK = 256
TOKENS = 8192


def draw_first_moment(key, part):
    key_one, key_two = jax.random.split(jax.random.fold_in(key, 11), 2)
    row_rise = jnp.arange(RANK, dtype=jnp.float32) / max(RANK - 1, 1)
    col_rise = jnp.arange(C, dtype=jnp.float32) / max(C - 1, 1)
    rise_table = jnp.exp(jnp.log(3.0) * row_rise)[:, None] * jnp.exp(jnp.log(3.0) * col_rise)[None, :]
    roughness = jnp.exp(jax.random.uniform(key_two, (3, RANK, C), jnp.float32, 0.0, jnp.log(2.0)))
    base_draw = jnp.clip(jax.random.normal(key_one, (3, RANK, C), jnp.float32), -4.0, 4.0)
    return (0.1 * base_draw * rise_table[None, :, :] * roughness).astype(jnp.float32)


def spiked(result, rng, source, target, blocks, factor):
    owner, partner = [(jnp.arange(result.shape[axis_at]) // (result.shape[axis_at] // blocks)).reshape([-1 if axis == axis_at else 1 for axis in range(result.ndim)]) for axis_at in (source, target)]
    chosen = jax.random.permutation(rng, blocks)[partner]
    strong = (owner == chosen) | (owner == (partner + blocks // 2) % blocks)
    return jnp.where(strong, factor * result, result)


def block_levels(stream_key, extent, cuts, least, largest):
    factor_of = 1.0
    for dim, parts in cuts:
        draws = jax.random.uniform(jax.random.fold_in(jax.random.fold_in(stream_key, 6), dim), (parts,), jnp.float32, least / len(cuts), largest / len(cuts))
        factor_of = factor_of * jnp.repeat(jnp.exp(draws), extent[dim] // parts).reshape((-1,) + (1,) * (len(extent) - 1 - dim))
    return factor_of


def centred(own_key, dims, deviation, bound, cuts=(), held_as=jnp.bfloat16):
    result = deviation * jax.random.normal(own_key, dims, jnp.float32)
    if cuts:
        result = result * block_levels(own_key, dims, cuts, -0.22, 0.18)
    return jnp.clip(result, -bound, bound).astype(held_as)


def gaussian_with(key, extent, width, limit, pieces, heavy, kind=jnp.bfloat16):
    array = width * jax.random.normal(key, extent, jnp.float32)
    if pieces:
        array = array * block_levels(key, extent, pieces, -0.22, 0.18)
    return jnp.clip(spiked(array, jax.random.fold_in(key, 3), *heavy), -limit, limit).astype(kind)


def setup_inputs(seed: int = 0) -> dict:
    keys = jax.random.split(jax.random.key(seed), 12)
    inputs = gaussian_with(keys[0], (TOKENS, D), 1.0, 8.0, ((0, 8),), (0, 1, 8, 2.0))
    value_cot = centred(keys[1], (TOKENS, C), (RANK ** 0.5 * (D * TOKENS) ** -0.5), 0.015625, ((0, 8), (1, 4)))
    gate_cot = centred(keys[2], (TOKENS, C), (RANK ** 0.5 * (D * TOKENS) ** -0.5), 0.015625, ((0, 8), (1, 4)))
    out_cot = gaussian_with(keys[3], (TOKENS, D), (RANK ** 0.5 * (D * TOKENS) ** -0.5), 0.0234375, ((0, 8),), (0, 1, 8, 2.0))
    conv_output = centred(keys[4], (TOKENS, C), 1.0, 6.0, ((0, 8), (1, 4)))
    factors = centred(keys[5], (3, D, RANK), RANK ** -0.5, 0.375, ((1, 8),))
    value_weight = centred(keys[6], (D, C), D ** -0.5, 0.09375, ((0, 8), (1, 4)), jnp.float32)
    gate_weight = centred(keys[7], (D, C), D ** -0.5, 0.09375, ((0, 8), (1, 4)), jnp.float32)
    out_weight = centred(keys[8], (C, D), C ** -0.5, 0.125, ((0, 4), (1, 8)), jnp.float32)
    first_moment = draw_first_moment(jax.random.fold_in(keys[11], 71), 0)
    second_moment = jnp.clip(jnp.exp(math.log(0.05) - 2.3025851 * jax.random.uniform(keys[10], (3, RANK, C), jnp.float32) ** block_levels(keys[10], (3, RANK, C), ((1, 8), (2, 4)), -0.2, 0.2)), 0.005, 0.05)
    return dict(inputs=inputs, value_cot=value_cot, gate_cot=gate_cot, out_cot=out_cot, conv_output=conv_output, factors=factors, value_weight=value_weight, gate_weight=gate_weight, out_weight=out_weight, first_moment=first_moment, second_moment=second_moment)


FIRST_DECAY = 0.9
SECOND_DECAY = 0.95
DIVISOR_EPS = 1e-08
SQUARE_EPS = 1e-06
LEARN_RATE = 0.01

def project_side(source, factor, target):
    left_proj = jnp.dot(source.astype(jnp.float32), factor.astype(jnp.float32), precision=lax.Precision.HIGHEST)
    return jnp.dot(left_proj.T, target.astype(jnp.float32), precision=lax.Precision.HIGHEST)

def reference(inputs, value_cot, gate_cot, out_cot, conv_output, factors, value_weight, gate_weight, out_weight, first_moment, second_moment):
    projected = jnp.stack([project_side(inputs, factors[0], value_cot), project_side(inputs, factors[1], gate_cot), project_side(out_cot, factors[2], conv_output)])
    new_first = FIRST_DECAY * first_moment + (1.0 - FIRST_DECAY) * projected
    new_second = SECOND_DECAY * second_moment + (1.0 - SECOND_DECAY) * projected * projected
    direction = new_first / (jnp.sqrt(new_second) + DIVISOR_EPS)
    total = jnp.sum(direction * direction)
    norm_scale = lax.rsqrt(total / (3 * RANK * C) + SQUARE_EPS)
    float_factors = factors.astype(jnp.float32)
    value_update = norm_scale * jnp.dot(float_factors[0], direction[0], precision=lax.Precision.HIGHEST)
    gate_update = norm_scale * jnp.dot(float_factors[1], direction[1], precision=lax.Precision.HIGHEST)
    out_update = (norm_scale * jnp.dot(float_factors[2], direction[2], precision=lax.Precision.HIGHEST)).T
    value_copy = (value_weight - LEARN_RATE * value_update).astype(jnp.bfloat16)
    gate_copy = (gate_weight - LEARN_RATE * gate_update).astype(jnp.bfloat16)
    out_copy = (out_weight - LEARN_RATE * out_update).astype(jnp.bfloat16)
    return (new_first, new_second, value_update, gate_update, out_update, value_copy, gate_copy, out_copy)
```

```python
import functools

import jax
import jax.numpy as jnp
from jax import lax
from jax.experimental import pallas as pl
from jax.experimental.pallas import tpu as pltpu
from jax.sharding import PartitionSpec as P

FIRST_DECAY = 0.9
SECOND_DECAY = 0.95
DIVISOR_EPS = 1e-08
SQUARE_EPS = 1e-06
LEARN_RATE = 0.01
K_STEP = 7.0
DIRECTION_GAIN = 512.0
VMEM_BYTES = 45 * 1024 * 1024
MESH = pl.DeviceIdType.MESH
F32 = jnp.float32
BF16 = jnp.bfloat16


def high_low(values):
    upper = values.astype(BF16)
    lower = (values - upper.astype(F32)).astype(BF16)
    return upper, lower


def others(coord, size, dist):
    if dist == 0:
        return [(coord, 0, None)]
    if size == 2:
        return [(1 - coord, None, None)]
    return [(coord - dist, -1, coord >= dist), (coord + dist, 1, coord + dist < size)]


def both(*preds):
    preds = [p for p in preds if p is not None]
    if not preds:
        return None
    return functools.reduce(jnp.logical_and, preds)


def run_if(pred, fn):
    if pred is None:
        fn()
    else:
        pl.when(pred)(fn)


def power(values):
    square = values * values
    return values * square * square * square


def encode(values, gain):
    return power(values * gain).astype(BF16)


def decode(coded, gain):
    value = coded.astype(F32)
    size = jnp.exp(jnp.log(jnp.abs(value)) * (1.0 / 7.0)) * (1.0 / gain)
    return jnp.where(value < 0.0, -size, size)


def stage_items(s, z_first, nz, nx, z, x):
    n1, n2 = (nz, nx) if z_first else (nx, nz)
    c1, c2 = (z, x) if z_first else (x, z)
    items = []
    for e in range(0, n2):
        d = s - e
        if d < 0 or d >= n1:
            continue
        for o1, s1, v1 in others(c1, n1, d):
            for o2, s2, v2 in others(c2, n2, e):
                slot = o1 * nx + o2 if z_first else o2 * nx + o1
                items.append((d, e, s1, s2, slot, both(v1, v2)))
    return items


def gather_sends(nz, nx):
    count = 0
    for c in range(6):
        n1, n2 = (nz, nx) if c else (nx, nz)
        for d in range(n1):
            firsts = [0] if d == 0 else ([None] if n1 == 2 else [-1, 1])
            for e in range(n2):
                seconds = [0] if e == 0 else ([None] if n2 == 2 else [-1, 1])
                for s1 in firsts:
                    for s2 in seconds:
                        if e == 0 and d < n1 - 1:
                            count += (s1 in (-1, 0)) + (s1 in (1, 0))
                        if e < n2 - 1:
                            count += (s2 in (-1, 0)) + (s2 in (1, 0))
    return count


def schedule(nz, nx):
    steps = []

    def add(at, name, *args):
        steps.append((at, name, args))

    add(0.0, "f_own_z", 0)
    add(0.0, "f_own_x", 0)
    add(0.1, "f_own_z", 1)
    add(0.2, "f_own_z", 2)
    for k in range(3):
        at = K_STEP * k
        if k:
            add(at, "f_own_x", k)
        add(2.5 + at, "own_part", k)
        for e in range(nx):
            for j in range(nz):
                if j or e:
                    there = at + 3.5 + (1.6 * (j - 1) if j else 0.0) + (3.4 if j and e else 0.0)
                    add(there, "f_arrive", k, j, e)
                    add(there + 2.9, "f_pass", k, j, e)
                    add(there + 4.4, "f_use", k, j, e)
        done = at + 3.5 + 1.6 * (nz - 2) + 3.4 + 4.5
        add(done, "split", k)
        add(done + 1.8, "partial", k)
        ready = done + 2.0
        for order, i in enumerate(list(range(1, nz)) + [0]):
            add(ready + 5.0 + 1.5 * order, "along_z", k, i)
        ready += 5.0 + 1.5 * nz + 3.0
        add(ready, "moments", k)
        for e in range(nx):
            for j in range(nz):
                if j or e:
                    add(ready + 2.5 + (1.0 * (j - 1) if j else 0.0) + (2.5 if j and e else 0.0), "d_arrive", k, j, e)
        add(ready + 9.0, "unscaled", k)
    add(ready + 2.4, "norm")
    steps.sort(key=lambda step: step[0])
    return steps


def kernel(
    nz, nx, tp, steps_of,
    x_hbm, oc_hbm, vc_hbm, gc_hbm, co_hbm, f_hbm, w0_hbm, w1_hbm, w2_hbm, m1_ref, m2_ref,
    nf_ref, ns_ref, u0_ref, u1_ref, u2_ref, c0_ref, c1_ref, c2_ref,
    x_v, oc_v, cots, fg, wts, acc, xf, part, rx, rz, q, dg, dh, dl, st, sf,
    in_sem, f_recv, y_recv, p_recv, xf_recv, rx_recv, rz_recv, d_recv, s_recv, c_recv, out_sem, c_send,
):
    me = lax.axis_index("fs")
    t = lax.axis_index("tp")
    z = lax.div(me, nx)
    x = lax.rem(me, nx)
    n = nz * nx
    core = lax.rem(t, 2)
    row = lax.rem(lax.div(t, 2), 2)
    mate = t + 1 - 2 * core
    beside = t + 2 - 4 * row
    block = f_hbm.shape[1]
    rank = f_hbm.shape[2]
    rows = m1_ref.shape[1]
    width = m1_ref.shape[2]
    own = x_v.shape[0]
    pending = []
    F_OUT, Y_OUT, P_OUT, XF_OUT, RX_OUT, RZ_OUT, D_OUT, ST_OUT, SF_OUT = range(9)

    def remote(src, dst, ssem, rsem, where):
        copy = pltpu.make_async_remote_copy(
            src_ref=src, dst_ref=dst, send_sem=ssem, recv_sem=rsem,
            device_id=where, device_id_type=MESH,
        )
        return copy

    def push(src, group, rsem, where, dst=None):
        remote(src, src if dst is None else dst, out_sem.at[group], rsem, where).start()

    def send(src, dst, rsem, where, pred, outer):
        copy = remote(src, dst, c_send.at[len(pending)], rsem, where)
        pred = both(pred, outer)
        run_if(pred, copy.start)
        pending.append((pred, copy))

    def arrived(dst, sem, pred=None):
        run_if(pred, pltpu.make_async_copy(dst, dst, sem).wait)

    mine = pl.ds(pl.multiple_of(core * own, own), own)
    theirs = pl.ds(pl.multiple_of((1 - core) * own, own), own)
    loads = [
        pltpu.make_async_copy(f_hbm, fg.at[:, me], in_sem.at[0]),
        pltpu.make_async_copy(x_hbm.at[mine], x_v, in_sem.at[1]),
        pltpu.make_async_copy(oc_hbm.at[mine], oc_v, in_sem.at[2]),
        pltpu.make_async_copy(vc_hbm, cots.at[0], in_sem.at[3]),
        pltpu.make_async_copy(gc_hbm, cots.at[1], in_sem.at[4]),
        pltpu.make_async_copy(co_hbm, cots.at[2], in_sem.at[5]),
        pltpu.make_async_copy(w0_hbm, wts[0], in_sem.at[6]),
        pltpu.make_async_copy(w1_hbm, wts[1], in_sem.at[7]),
        pltpu.make_async_copy(w2_hbm, wts[2], in_sem.at[8]),
    ]
    for load in loads:
        load.start()

    barrier = pltpu.get_barrier_semaphore()
    everyone = [{"fs": lax.rem(me + k, n)} for k in range(1, n)]
    everyone += [{"tp": lax.rem(t + k, tp)} for k in range(1, tp)]
    for peer in everyone:
        pl.semaphore_signal(barrier, inc=1, device_id=peer, device_id_type=MESH)
    with jax.named_scope("barrier"):
        pl.semaphore_wait(barrier, len(everyone))

    def ranked(j):
        near = [sorted((abs(i - c), i) for i in range(nz))[j][1] for c in range(nz)]
        peer = near[0]
        for c in range(1, nz):
            peer = jnp.where(z == c, near[c], peer)
        return peer

    zs = [ranked(j) for j in range(nz)]
    xs = [lax.rem(x + e, nx) for e in range(nx)]

    def slot_of(j, e):
        return zs[j] * nx + xs[e] if j or e else me

    unit = block // 16
    half = core * (block // 2)
    fs_start = pl.multiple_of(half + row * 3 * unit, unit)
    y_send_start = pl.multiple_of(half + row * 5 * unit, unit)
    y_recv_start = pl.multiple_of(half + (1 - row) * 5 * unit, unit)
    mate_half = pl.multiple_of((1 - core) * (block // 2), block // 2)

    def f_part(k, slot, start, size):
        return fg.at[k, slot, pl.ds(start, size), :]

    sources = (x_v, x_v, oc_v)

    def matmul(k, slot, first):
        cols = pl.ds(pl.multiple_of(slot * block, block), block)
        tile = 256

        def body(i, carry):
            r = pl.ds(pl.multiple_of(i * tile, tile), tile)
            prod = jnp.dot(sources[k][r, cols], fg[k, slot], preferred_element_type=F32)
            if first:
                acc[k, r, :] = prod
            else:
                acc[k, r, :] += prod
            return carry

        lax.fori_loop(0, own // tile, body, 0)

    def f_own_z(k):
        piece = f_part(k, me, fs_start, 5 * unit)
        for j in range(1, nz):
            push(piece, F_OUT, f_recv.at[k, me], {"fs": slot_of(j, 0)})

    def f_own_x(k):
        piece = f_part(k, me, fs_start, 5 * unit)
        for e in range(1, nx):
            push(piece, F_OUT, f_recv.at[k, me], {"fs": slot_of(0, e)})

    def f_arrive(k, j, e):
        slot = slot_of(j, e)
        piece = f_part(k, slot, fs_start, 5 * unit)
        arrived(piece, f_recv.at[k, slot])
        if e == 0:
            for other in range(1, nx):
                push(piece, F_OUT, f_recv.at[k, slot], {"fs": slot_of(0, other)})
        push(f_part(k, slot, y_send_start, 3 * unit), Y_OUT, y_recv.at[k, slot], {"tp": beside})
        push(piece, P_OUT, p_recv.at[k, slot], {"tp": mate})

    def f_pass(k, j, e):
        slot = slot_of(j, e)
        piece = f_part(k, slot, y_recv_start, 3 * unit)
        arrived(piece, y_recv.at[k, slot])
        push(piece, P_OUT, p_recv.at[k, slot], {"tp": mate})

    def f_use(k, j, e):
        slot = slot_of(j, e)
        arrived(f_part(k, slot, mate_half, block // 2), p_recv.at[k, slot])
        matmul(k, slot, False)

    def own_part(k):
        if k != 1:
            loads[1 + k // 2].wait()
        matmul(k, me, True)

    dims = (((0,), (0,)), ((), ()))

    def product(k, r):
        prod = lax.dot_general(xf[k, 0, r, :], cots[k, r, :], dims, preferred_element_type=F32)
        prod = prod + lax.dot_general(xf[k, 1, r, :], cots[k, r, :], dims, preferred_element_type=F32)
        return prod.reshape(n, rows, width)

    def split(k):
        upper, lower = high_low(acc[k])
        xf[k, 0, mine, :] = upper
        xf[k, 1, mine, :] = lower
        push(xf.at[k, :, mine, :], XF_OUT, xf_recv.at[k], {"tp": mate})
        loads[3 + k].wait()
        part[k] = product(k, mine)

    order = list(range(1, nz)) + [0]

    def partial(k):
        arrived(xf.at[k, :, theirs, :], xf_recv.at[k])
        part[k] = part[k] + product(k, theirs)
        for i in order:
            oz = lax.rem(z + i, nz)
            for e in range(1, nx):
                slot = oz * nx + xs[e]
                push(part.at[k, slot], RX_OUT, rx_recv.at[k, e - 1, i], {"fs": z * nx + xs[e]}, rx.at[k, e - 1, i])

    def along_z(k, i):
        oz = lax.rem(z + i, nz)
        value = part[k, oz * nx + x]
        for e in range(1, nx):
            arrived(rx.at[k, e - 1, i], rx_recv.at[k, e - 1, i])
            value = value + rx[k, e - 1, i]
        q[k, i] = value
        if i:
            push(q.at[k, i], RZ_OUT, rz_recv.at[k, i - 1], {"fs": oz * nx + x}, rz.at[k, i - 1])

    def moments(k):
        projected = q[k, 0]
        for i in range(1, nz):
            arrived(rz.at[k, i - 1], rz_recv.at[k, i - 1])
            projected = projected + rz[k, i - 1]
        new_first = FIRST_DECAY * m1_ref[k] + (1.0 - FIRST_DECAY) * projected
        new_second = SECOND_DECAY * m2_ref[k] + (1.0 - SECOND_DECAY) * projected * projected
        nf_ref[k] = new_first
        ns_ref[k] = new_second
        direction = new_first / (jnp.sqrt(new_second) + DIVISOR_EPS)
        dg[k, me] = encode(direction, DIRECTION_GAIN)
        piece = dg.at[k, me]
        for j in range(nz - 1, 0, -1):
            push(piece, D_OUT, d_recv.at[k, me], {"fs": slot_of(j, 0)})
        for e in range(1, nx):
            push(piece, D_OUT, d_recv.at[k, me], {"fs": slot_of(0, e)})
        square = jnp.sum((direction * direction).reshape(rows * width // 1024, 8, 128), axis=0)
        st[0] = square if k == 0 else st[0] + square
        if k == 2:
            for i in range(1, tp):
                push(st.at[0], ST_OUT, s_recv.at[0], {"tp": lax.rem(t + i, tp)}, st.at[tp - i])

    def norm():
        arrived(st.at[pl.ds(1, tp - 1)], s_recv.at[0])
        value = st[0]
        for i in range(1, tp):
            value = value + st[i]
        sf[0] = value
        for i in range(1, n):
            push(sf.at[0], SF_OUT, s_recv.at[1], {"fs": lax.rem(me + i, n)}, sf.at[n - i])

    def d_arrive(k, j, e):
        slot = slot_of(j, e)
        piece = dg.at[k, slot]
        arrived(piece, d_recv.at[k, slot])
        if e == 0:
            for other in range(1, nx):
                push(piece, D_OUT, d_recv.at[k, slot], {"fs": slot_of(0, other)})

    tdims = (((0,), (1,)), ((), ()))
    news = (u0_ref, u1_ref, u2_ref)

    def unscaled(k):
        value = decode(dg[k].reshape(rank, width), DIRECTION_GAIN)
        upper, lower = high_low(value)
        dh[k] = upper
        dl[k] = lower
        if k < 2:
            news[k][...] = jnp.dot(fg[k, me], dh[k], preferred_element_type=F32) + jnp.dot(
                fg[k, me], dl[k], preferred_element_type=F32
            )
        else:
            news[k][...] = lax.dot_general(dh[k], fg[k, me], tdims, preferred_element_type=F32) + lax.dot_general(
                dl[k], fg[k, me], tdims, preferred_element_type=F32
            )

    table = dict(
        f_own_z=f_own_z, f_own_x=f_own_x, f_arrive=f_arrive, f_pass=f_pass, f_use=f_use, own_part=own_part,
        split=split, partial=partial, along_z=along_z, moments=moments, d_arrive=d_arrive, norm=norm,
        unscaled=unscaled,
    )
    loads[0].wait()
    for _, name, args in steps_of:
        with jax.named_scope(name + "_" + "_".join(str(v) for v in args)):
            table[name](*args)

    for load in loads[6:9]:
        load.wait()
    with jax.named_scope("total"):
        arrived(sf.at[pl.ds(1, n - 1)], s_recv.at[1])
        sums = sf[0]
        for i in range(1, n):
            sums = sums + sf[i]
        total = jnp.sum(jnp.sum(sums, axis=0, keepdims=True), axis=1, keepdims=True)
        scale = lax.rsqrt(total / (3 * rank * width * tp) + SQUARE_EPS)

    outs = (c0_ref, c1_ref, c2_ref)
    chunks = [(m, h) for m in range(3) for h in range(2)]

    def place(m, h, slot):
        if m < 2:
            size = block // 2
            return outs[m].at[pl.ds(pl.multiple_of(slot * block + h * size, size), size), :]
        size = width // 2
        return outs[m].at[pl.ds(h * size, size), pl.ds(pl.multiple_of(slot * block, block), block)]

    def forward(item, z_first, src, rsem):
        d, e, s1, s2, slot, valid = item
        n1, n2 = (nz, nx) if z_first else (nx, nz)
        c1, c2 = (z, x) if z_first else (x, z)
        st1, st2 = (nx, 1) if z_first else (1, nx)
        if e == 0 and d < n1 - 1:
            if s1 in (-1, 0):
                send(src, src, rsem, {"fs": me + st1}, c1 + 1 < n1, valid)
            if s1 in (1, 0):
                send(src, src, rsem, {"fs": me - st1}, c1 > 0, valid)
        if e < n2 - 1:
            if s2 in (-1, 0):
                send(src, src, rsem, {"fs": me + st2}, c2 + 1 < n2, valid)
            if s2 in (1, 0):
                send(src, src, rsem, {"fs": me - st2}, c2 > 0, valid)

    for s in range(nz + nx - 1):
        for c, (m, h) in enumerate(chunks):
            z_first = c > 0
            if s == 0:
                size = (block if m < 2 else width) // 2
                r = pl.ds(h * size, size)
                update = scale * news[m][r, :]
                news[m][r, :] = update
                place(m, h, me)[...] = (wts[m][r, :] - LEARN_RATE * update).astype(BF16)
            with jax.named_scope(f"gather_{s}_{c}"):
                for item in stage_items(s, z_first, nz, nx, z, x):
                    slot, valid = item[4], item[5]
                    dst = place(m, h, slot)
                    if s > 0:
                        arrived(dst, c_recv.at[c, slot], valid)
                    forward(item, z_first, dst, c_recv.at[c, slot])
    with jax.named_scope("drain"):
        for pred, copy in pending:
            run_if(pred, copy.wait_send)
        last = pl.ds(0, n - 1)
        arrived(fg.at[:, last, pl.ds(0, 5 * unit), :], out_sem.at[F_OUT])
        arrived(fg.at[:, last, pl.ds(0, 3 * unit), :], out_sem.at[Y_OUT])
        arrived(fg.at[:, last, pl.ds(0, block // 2), :], out_sem.at[P_OUT])
        arrived(xf.at[:, :, mine, :], out_sem.at[XF_OUT])
        arrived(part.at[:, pl.ds(0, nz * (nx - 1))], out_sem.at[RX_OUT])
        arrived(rz, out_sem.at[RZ_OUT])
        arrived(dg.at[:, last], out_sem.at[D_OUT])
        arrived(st.at[pl.ds(1, tp - 1)], out_sem.at[ST_OUT])
        arrived(sf.at[pl.ds(1, n - 1)], out_sem.at[SF_OUT])


def store_kernel(*refs):
    count = (len(refs) - 1) // 2
    sems = refs[-1]
    copies = [pltpu.make_async_copy(refs[i], refs[count + i], sems.at[i]) for i in range(count)]
    for copy in copies:
        copy.start()
    for copy in copies:
        copy.wait()


def shards(nz, nx, tp, *args):
    inputs, value_cot, gate_cot, out_cot, conv_output, factors, vw, gw, ow, m1, m2 = args
    n = nz * nx
    block, rank = factors.shape[1], factors.shape[2]
    rows, width = m1.shape[1], m1.shape[2]
    tokens = inputs.shape[0]
    features = inputs.shape[1]
    any_ = pl.BlockSpec(memory_space=pl.ANY)
    vmem = pl.BlockSpec(memory_space=pltpu.VMEM)
    dma = pltpu.SemaphoreType.DMA
    own = tokens // 2
    scratch = [
        pltpu.VMEM((own, features), BF16),
        pltpu.VMEM((own, features), BF16),
        pltpu.VMEM((3, tokens, width), BF16),
        pltpu.VMEM((3, n, block, rank), BF16),
        (pltpu.VMEM(vw.shape, F32), pltpu.VMEM(gw.shape, F32), pltpu.VMEM(ow.shape, F32)),
        pltpu.VMEM((3, own, rank), F32),
        pltpu.VMEM((3, 2, tokens, rank), BF16),
        pltpu.VMEM((3, n, rows, width), F32),
        pltpu.VMEM((3, nx - 1, nz, rows, width), F32),
        pltpu.VMEM((3, nz - 1, rows, width), F32),
        pltpu.VMEM((3, nz, rows, width), F32),
        pltpu.VMEM((3, n, rows, width), BF16),
        pltpu.VMEM((3, rank, width), BF16),
        pltpu.VMEM((3, rank, width), BF16),
        pltpu.VMEM((tp, 8, 128), F32),
        pltpu.VMEM((n, 8, 128), F32),
        dma((9,)),
        dma((3, n)), dma((3, n)), dma((3, n)), dma((3,)),
        dma((3, nx - 1, nz)), dma((3, nz - 1)), dma((3, n)), dma((2,)), dma((6, n)),
        dma((9,)), dma((gather_sends(nz, nx),)),
    ]
    shape = [
        (m1.shape, F32), (m2.shape, F32), (vw.shape, F32), (gw.shape, F32), (ow.shape, F32),
        ((features, width), BF16), ((features, width), BF16), ((width, features), BF16),
    ]
    held = pl.pallas_call(
        functools.partial(kernel, nz, nx, tp, schedule(nz, nx)),
        out_shape=tuple(pltpu.VMEM(*item) for item in shape),
        in_specs=[any_] * 9 + [vmem] * 2,
        out_specs=(vmem,) * 8,
        scratch_shapes=scratch,
        compiler_params=pltpu.CompilerParams(
            collective_id=0, has_side_effects=True, vmem_limit_bytes=VMEM_BYTES
        ),
    )(inputs, out_cot, value_cot, gate_cot, conv_output, factors, vw, gw, ow, m1, m2)
    return pl.pallas_call(
        store_kernel,
        out_shape=tuple(jax.ShapeDtypeStruct(*item) for item in shape),
        in_specs=[vmem] * 8,
        out_specs=(any_,) * 8,
        scratch_shapes=[dma((8,))],
        compiler_params=pltpu.CompilerParams(vmem_limit_bytes=1024 * 1024),
    )(*held)


def solution(mesh):
    fs, tp = mesh.shape["fs"], mesh.shape["tp"]
    nz = 1 << (fs.bit_length() // 2)
    nx = fs // nz
    placed = (
        P("fs", None),
        P("fs", "tp"),
        P("fs", "tp"),
        P("fs", None),
        P("fs", "tp"),
        P(None, "fs", None),
        P("fs", "tp"),
        P("fs", "tp"),
        P("tp", "fs"),
        P(None, "fs", "tp"),
        P(None, "fs", "tp"),
    )
    return jax.shard_map(
        functools.partial(shards, nz, nx, tp),
        mesh=mesh,
        in_specs=placed,
        out_specs=(
            P(None, "fs", "tp"),
            P(None, "fs", "tp"),
            P("fs", "tp"),
            P("fs", "tp"),
            P("tp", "fs"),
            P(None, "tp"),
            P(None, "tp"),
            P("tp", None),
        ),
        check_vma=False,
    )
```

```python
import functools

import jax
import jax.numpy as jnp
from jax import lax
from jax.experimental import pallas as pl
from jax.experimental.pallas import tpu as pltpu
from jax.sharding import PartitionSpec as P

FIRST_DECAY = 0.9
SECOND_DECAY = 0.95
DIVISOR_EPS = 1e-08
SQUARE_EPS = 1e-06
LEARN_RATE = 0.01
K_STEP = 7.0
USE_LAG = 6.5
DIRECTION_GAIN = 128.0
WEIGHT_GAIN = 65536.0
EARLY = 8
PARTIAL = (24.0, 28.0, 36.0)
ALONG_Z = (28.6, 36.5, 42.5)
ALONG_STEP = (1.0, 0.3, 1.0)
MOMENTS = (38.0, 47.5, 51.0)
EARLY_Z = (20.0, 53.5, 53.6)
EARLY_X = (39.0, 39.5, 39.6)
LATE = (1, 2)
GATHER_D = (48.0, 51.1, 54.5)
LAST_D = (52.0, 55.5, 57.5)
VMEM_BYTES = 45 * 1024 * 1024
MESH = pl.DeviceIdType.MESH
F32 = jnp.float32
BF16 = jnp.bfloat16


def high_low(values):
    upper = values.astype(BF16)
    lower = (values - upper.astype(F32)).astype(BF16)
    return upper, lower


def others(coord, size, dist):
    if dist == 0:
        return [(coord, 0, None)]
    if size == 2:
        return [(1 - coord, None, None)]
    return [(coord - dist, -1, coord >= dist), (coord + dist, 1, coord + dist < size)]


def both(*preds):
    preds = [p for p in preds if p is not None]
    if not preds:
        return None
    return functools.reduce(jnp.logical_and, preds)


def run_if(pred, fn):
    if pred is None:
        fn()
    else:
        pl.when(pred)(fn)


def power(values):
    cube = values * values * values
    return cube * cube * cube


def encode(values, gain):
    return power(values * gain).astype(BF16)


def decode(coded, gain):
    value = coded.astype(F32)
    size = jnp.exp(jnp.log(jnp.abs(value)) * (1.0 / 9.0)) * (1.0 / gain)
    return jnp.where(value < 0.0, -size, size)


def stage_items(s, z_first, nz, nx, z, x):
    n1, n2 = (nz, nx) if z_first else (nx, nz)
    c1, c2 = (z, x) if z_first else (x, z)
    items = []
    for e in range(0, n2):
        d = s - e
        if d < 0 or d >= n1:
            continue
        for o1, s1, v1 in others(c1, n1, d):
            for o2, s2, v2 in others(c2, n2, e):
                slot = o1 * nx + o2 if z_first else o2 * nx + o1
                items.append((d, e, s1, s2, slot, both(v1, v2)))
    return items


def gather_sends(nz, nx, z, x, z_first):
    n1, n2 = (nz, nx) if z_first else (nx, nz)
    c1, c2 = (z, x) if z_first else (x, z)
    count = 0
    for o1 in range(n1):
        for o2 in range(n2):
            if o2 == c2:
                count += (o1 <= c1 < n1 - 1) + (o1 >= c1 > 0)
            count += (o2 <= c2 < n2 - 1) + (o2 >= c2 > 0)
    return count


def schedule(nz, nx):
    steps = []

    def add(at, name, *args):
        steps.append((at, name, args))

    def pieces(name, k, first, apart, behind, last):
        for e in range(nx):
            for j in range(nz):
                if j and not e:
                    add(first + apart * (j - 1), name, k, j, e)
                elif e:
                    add(behind if j == 0 else last + 0.4 * j, name, k, j, e)

    for k in range(3):
        at = K_STEP * k
        add(0.01 * k, "f_own_x", k)
        add(max(at - 0.5, 0.0), "f_own_z", k)
        add(2.5 + at, "own_part", k)
        for e in range(nx):
            for j in range(nz):
                if j or e:
                    if j == 0:
                        there = 4.0 + 1.8 * k
                    else:
                        there = at + (5.0, 7.5, 9.0)[j - 1] + (4.0 if e else 0.0)
                    add(there, "f_arrive", k, j, e)
                    add(there + 3.2, "f_pass", k, j, e)
                    add(max(there + USE_LAG, at + 6.0), "f_use", k, j, e)
        add(at + 13.3 + USE_LAG, "split", k)
        add(PARTIAL[k], "partial", k)
        for step, i in enumerate(list(range(1, nz)) + [0]):
            add(ALONG_Z[k] + ALONG_STEP[k] * step, "along_z", k, i)
        add(MOMENTS[k], "moments", k)
        pieces("d_arrive", k, GATHER_D[k], 0.3, GATHER_D[k] + 0.1, LAST_D[k])
        add(LAST_D[k] + 2.0, "unscaled", k)
    add(MOMENTS[2] + 1.5, "norm")
    for m in range(3):
        add(3.0, "e_code", m)
        add(EARLY_Z[m], "e_own_z", m)
        add(EARLY_X[m], "e_own_x", m)
        if m not in LATE:
            for j in range(1, nz):
                add(EARLY_X[m] + 0.1, "e_arrive", m, j)
    steps.sort(key=lambda step: step[0])
    return steps


def kernel(
    nz, nx, tp, steps_of,
    x_hbm, oc_hbm, vc_hbm, gc_hbm, co_hbm, f_hbm, w0_hbm, w1_hbm, w2_hbm, m1_ref, m2_ref,
    nf_ref, ns_ref, u0_ref, u1_ref, u2_ref, c0_ref, c1_ref, c2_ref,
    x_v, oc_v, cots, fg, wts, acc, xf, part, rx, rz, q, dg, dh, dl, st, sf, early,
    in_sem, f_recv, y_recv, p_recv, xf_recv, rx_recv, rz_recv, d_recv, s_recv, c_recv, out_sem, c_send, e_recv, e_send,
):
    me = lax.axis_index("fs")
    t = lax.axis_index("tp")
    z = lax.div(me, nx)
    x = lax.rem(me, nx)
    n = nz * nx
    core = lax.rem(t, 2)
    row = lax.rem(lax.div(t, 2), 2)
    mate = t + 1 - 2 * core
    beside = t + 2 - 4 * row
    block = f_hbm.shape[1]
    rank = f_hbm.shape[2]
    rows = m1_ref.shape[1]
    width = m1_ref.shape[2]
    own = x_v.shape[0]
    F_OUT, Y_OUT, P_OUT, XF_OUT, RX_OUT, RZ_OUT, D_OUT, ST_OUT, SF_OUT = range(9)

    def remote(src, dst, ssem, rsem, where):
        copy = pltpu.make_async_remote_copy(
            src_ref=src, dst_ref=dst, send_sem=ssem, recv_sem=rsem,
            device_id=where, device_id_type=MESH,
        )
        return copy

    def push(src, group, rsem, where, dst=None):
        remote(src, src if dst is None else dst, out_sem.at[group], rsem, where).start()

    def send(src, ssem, rsem, where, pred, outer):
        run_if(both(pred, outer), remote(src, src, ssem, rsem, where).start)

    def arrived(dst, sem, pred=None):
        run_if(pred, pltpu.make_async_copy(dst, dst, sem).wait)

    mine = pl.ds(pl.multiple_of(core * own, own), own)
    theirs = pl.ds(pl.multiple_of((1 - core) * own, own), own)
    loads = [
        pltpu.make_async_copy(f_hbm, fg.at[:, me], in_sem.at[0]),
        pltpu.make_async_copy(x_hbm.at[mine], x_v, in_sem.at[1]),
        pltpu.make_async_copy(oc_hbm.at[mine], oc_v, in_sem.at[2]),
        pltpu.make_async_copy(vc_hbm, cots.at[0], in_sem.at[3]),
        pltpu.make_async_copy(gc_hbm, cots.at[1], in_sem.at[4]),
        pltpu.make_async_copy(co_hbm, cots.at[2], in_sem.at[5]),
        pltpu.make_async_copy(w0_hbm, wts[0], in_sem.at[6]),
        pltpu.make_async_copy(w1_hbm, wts[1], in_sem.at[7]),
        pltpu.make_async_copy(w2_hbm, wts[2], in_sem.at[8]),
    ]
    for load in loads:
        load.start()

    barrier = pltpu.get_barrier_semaphore()
    everyone = [{"fs": lax.rem(me + k, n)} for k in range(1, n)]
    everyone += [{"tp": lax.rem(t + k, tp)} for k in range(1, tp)]
    for peer in everyone:
        pl.semaphore_signal(barrier, inc=1, device_id=peer, device_id_type=MESH)
    with jax.named_scope("barrier"):
        pl.semaphore_wait(barrier, len(everyone))

    def ranked(j):
        near = [sorted((abs(i - c), i) for i in range(nz))[j][1] for c in range(nz)]
        peer = near[0]
        for c in range(1, nz):
            peer = jnp.where(z == c, near[c], peer)
        return peer

    zs = [ranked(j) for j in range(nz)]
    xs = [lax.rem(x + e, nx) for e in range(nx)]

    def slot_of(j, e):
        return zs[j] * nx + xs[e] if j or e else me

    unit = block // 16
    half = core * (block // 2)
    fs_start = pl.multiple_of(half + row * 3 * unit, unit)
    y_send_start = pl.multiple_of(half + row * 5 * unit, unit)
    y_recv_start = pl.multiple_of(half + (1 - row) * 5 * unit, unit)
    mate_half = pl.multiple_of((1 - core) * (block // 2), block // 2)

    def f_part(k, slot, start, size):
        return fg.at[k, slot, pl.ds(start, size), :]

    sources = (x_v, x_v, oc_v)
    spans = [(wide // EARLY, (wide - wide // EARLY) // 2) for wide in (block, block, width)]

    def e_push(m, slot, where):
        piece = early[m].at[slot]
        remote(piece, piece, e_send.at[m], e_recv.at[m, slot], {"fs": where}).start()

    def e_code(m):
        loads[6 + m].wait()
        early[m][me] = encode(wts[m][pl.ds(0, spans[m][0]), :], WEIGHT_GAIN)

    def e_own_z(m):
        for j in range(nz - 1, 0, -1):
            e_push(m, me, slot_of(j, 0))

    def e_own_x(m):
        for e in range(1, nx):
            e_push(m, me, slot_of(0, e))

    def e_arrive(m, j):
        slot = slot_of(j, 0)
        arrived(early[m].at[slot], e_recv.at[m, slot])
        for e in range(1, nx):
            e_push(m, slot, slot_of(0, e))

    def matmul(k, slot, first):
        cols = pl.ds(pl.multiple_of(slot * block, block), block)
        tile = 256

        def body(i, carry):
            r = pl.ds(pl.multiple_of(i * tile, tile), tile)
            prod = jnp.dot(sources[k][r, cols], fg[k, slot], preferred_element_type=F32)
            if first:
                acc[k, r, :] = prod
            else:
                acc[k, r, :] += prod
            return carry

        lax.fori_loop(0, own // tile, body, 0)

    def f_own_z(k):
        piece = f_part(k, me, fs_start, 5 * unit)
        for j in range(1, nz):
            push(piece, F_OUT, f_recv.at[k, me], {"fs": slot_of(j, 0)})

    def f_own_x(k):
        piece = f_part(k, me, fs_start, 5 * unit)
        for e in range(1, nx):
            push(piece, F_OUT, f_recv.at[k, me], {"fs": slot_of(0, e)})

    def f_arrive(k, j, e):
        slot = slot_of(j, e)
        piece = f_part(k, slot, fs_start, 5 * unit)
        arrived(piece, f_recv.at[k, slot])
        if e == 0:
            for other in range(1, nx):
                push(piece, F_OUT, f_recv.at[k, slot], {"fs": slot_of(0, other)})
        push(f_part(k, slot, y_send_start, 3 * unit), Y_OUT, y_recv.at[k, slot], {"tp": beside})
        push(piece, P_OUT, p_recv.at[k, slot], {"tp": mate})

    def f_pass(k, j, e):
        slot = slot_of(j, e)
        piece = f_part(k, slot, y_recv_start, 3 * unit)
        arrived(piece, y_recv.at[k, slot])
        push(piece, P_OUT, p_recv.at[k, slot], {"tp": mate})

    def f_use(k, j, e):
        slot = slot_of(j, e)
        arrived(f_part(k, slot, mate_half, block // 2), p_recv.at[k, slot])
        matmul(k, slot, False)

    def own_part(k):
        if k != 1:
            loads[1 + k // 2].wait()
        matmul(k, me, True)

    dims = (((0,), (0,)), ((), ()))

    def product(k, r):
        prod = lax.dot_general(xf[k, 0, r, :], cots[k, r, :], dims, preferred_element_type=F32)
        prod = prod + lax.dot_general(xf[k, 1, r, :], cots[k, r, :], dims, preferred_element_type=F32)
        return prod.reshape(n, rows, width)

    def split(k):
        upper, lower = high_low(acc[k])
        xf[k, 0, mine, :] = upper
        xf[k, 1, mine, :] = lower
        push(xf.at[k, :, mine, :], XF_OUT, xf_recv.at[k], {"tp": mate})
        loads[3 + k].wait()
        part[k] = product(k, mine)

    order = list(range(1, nz)) + [0]

    def partial(k):
        arrived(xf.at[k, :, theirs, :], xf_recv.at[k])
        part[k] = part[k] + product(k, theirs)
        for i in order:
            oz = lax.rem(z + i, nz)
            for e in range(1, nx):
                slot = oz * nx + xs[e]
                push(part.at[k, slot], RX_OUT, rx_recv.at[k, e - 1, i], {"fs": z * nx + xs[e]}, rx.at[k, e - 1, i])

    def along_z(k, i):
        oz = lax.rem(z + i, nz)
        value = part[k, oz * nx + x]
        for e in range(1, nx):
            arrived(rx.at[k, e - 1, i], rx_recv.at[k, e - 1, i])
            value = value + rx[k, e - 1, i]
        q[k, i] = value
        if i:
            push(q.at[k, i], RZ_OUT, rz_recv.at[k, i - 1], {"fs": oz * nx + x}, rz.at[k, i - 1])

    def moments(k):
        projected = q[k, 0]
        for i in range(1, nz):
            arrived(rz.at[k, i - 1], rz_recv.at[k, i - 1])
            projected = projected + rz[k, i - 1]
        new_first = FIRST_DECAY * m1_ref[k] + (1.0 - FIRST_DECAY) * projected
        new_second = SECOND_DECAY * m2_ref[k] + (1.0 - SECOND_DECAY) * projected * projected
        nf_ref[k] = new_first
        ns_ref[k] = new_second
        direction = new_first / (jnp.sqrt(new_second) + DIVISOR_EPS)
        dg[k, me] = encode(direction, DIRECTION_GAIN)
        piece = dg.at[k, me]
        for j in range(nz - 1, 0, -1):
            push(piece, D_OUT, d_recv.at[k, me], {"fs": slot_of(j, 0)})
        for e in range(1, nx):
            push(piece, D_OUT, d_recv.at[k, me], {"fs": slot_of(0, e)})
        square = jnp.sum((direction * direction).reshape(rows * width // 1024, 8, 128), axis=0)
        st[0] = square if k == 0 else st[0] + square
        if k == 2:
            for i in range(1, tp):
                push(st.at[0], ST_OUT, s_recv.at[0], {"tp": lax.rem(t + i, tp)}, st.at[tp - i])

    def norm():
        arrived(st.at[pl.ds(1, tp - 1)], s_recv.at[0])
        value = st[0]
        for i in range(1, tp):
            value = value + st[i]
        sf[0] = value
        for i in range(1, n):
            push(sf.at[0], SF_OUT, s_recv.at[1], {"fs": lax.rem(me + i, n)}, sf.at[n - i])

    def d_arrive(k, j, e):
        slot = slot_of(j, e)
        piece = dg.at[k, slot]
        arrived(piece, d_recv.at[k, slot])
        if e == 0:
            for other in range(1, nx):
                push(piece, D_OUT, d_recv.at[k, slot], {"fs": slot_of(0, other)})

    tdims = (((0,), (1,)), ((), ()))
    news = (u0_ref, u1_ref, u2_ref)

    def unscaled(k):
        value = decode(dg[k].reshape(rank, width), DIRECTION_GAIN)
        upper, lower = high_low(value)
        dh[k] = upper
        dl[k] = lower
        if k < 2:
            news[k][...] = jnp.dot(fg[k, me], dh[k], preferred_element_type=F32) + jnp.dot(
                fg[k, me], dl[k], preferred_element_type=F32
            )
        else:
            news[k][...] = lax.dot_general(dh[k], fg[k, me], tdims, preferred_element_type=F32) + lax.dot_general(
                dl[k], fg[k, me], tdims, preferred_element_type=F32
            )

    table = dict(
        f_own_z=f_own_z, f_own_x=f_own_x, f_arrive=f_arrive, f_pass=f_pass, f_use=f_use, own_part=own_part,
        split=split, partial=partial, along_z=along_z, moments=moments, d_arrive=d_arrive, norm=norm,
        unscaled=unscaled, e_code=e_code, e_own_z=e_own_z, e_own_x=e_own_x, e_arrive=e_arrive,
    )
    loads[0].wait()
    for _, name, args in steps_of:
        with jax.named_scope(name + "_" + "_".join(str(v) for v in args)):
            table[name](*args)

    with jax.named_scope("total"):
        arrived(sf.at[pl.ds(1, n - 1)], s_recv.at[1])
        sums = sf[0]
        for i in range(1, n):
            sums = sums + sf[i]
        total = jnp.sum(jnp.sum(sums, axis=0, keepdims=True), axis=1, keepdims=True)
        scale = lax.rsqrt(total / (3 * rank * width * tp) + SQUARE_EPS)

    outs = (c0_ref, c1_ref, c2_ref)
    chunks = [(m, h) for m in range(3) for h in range(2)]
    others_first = [(m, j, e) for e in range(nx) for j in range(nz) if j or e for m in range(3)]

    def place(m, start, size, slot):
        if m < 2:
            return outs[m].at[pl.ds(pl.multiple_of(slot * block + start, 16), size), :]
        return outs[m].at[pl.ds(start, size), pl.ds(pl.multiple_of(slot * block, block), block)]

    def settle(m, start, size):
        r = pl.ds(start, size)
        update = scale * news[m][r, :]
        news[m][r, :] = update
        place(m, start, size, me)[...] = (wts[m][r, :] - LEARN_RATE * update).astype(BF16)

    def complete(m, j, e):
        slot = slot_of(j, e)
        first = spans[m][0]
        if e:
            arrived(early[m].at[slot], e_recv.at[m, slot])
        if m < 2:
            rows_in = fg[m, slot, pl.ds(0, first), :]
            update = jnp.dot(rows_in, dh[m], preferred_element_type=F32)
            update = update + jnp.dot(rows_in, dl[m], preferred_element_type=F32)
        else:
            cols = pl.ds(0, first)
            update = lax.dot_general(dh[2, :, cols], fg[2, slot], tdims, preferred_element_type=F32)
            update = update + lax.dot_general(dl[2, :, cols], fg[2, slot], tdims, preferred_element_type=F32)
        weight = decode(early[m][slot], WEIGHT_GAIN)
        place(m, 0, first, slot)[...] = (weight - LEARN_RATE * (scale * update)).astype(BF16)

    def forward(item, z_first, src, ssem, rsem):
        d, e, s1, s2, slot, valid = item
        n1, n2 = (nz, nx) if z_first else (nx, nz)
        c1, c2 = (z, x) if z_first else (x, z)
        st1, st2 = (nx, 1) if z_first else (1, nx)
        if e == 0 and d < n1 - 1:
            if s1 in (-1, 0):
                send(src, ssem, rsem, {"fs": me + st1}, c1 + 1 < n1, valid)
            if s1 in (1, 0):
                send(src, ssem, rsem, {"fs": me - st1}, c1 > 0, valid)
        if e < n2 - 1:
            if s2 in (-1, 0):
                send(src, ssem, rsem, {"fs": me + st2}, c2 + 1 < n2, valid)
            if s2 in (1, 0):
                send(src, ssem, rsem, {"fs": me - st2}, c2 > 0, valid)

    stages = nz + nx - 1
    each = -(-len(others_first) // (len(chunks) * (stages - 3)))
    for s in range(stages):
        for c, (m, h) in enumerate(chunks):
            z_first = c > 0
            first, size = spans[m]
            start = first + h * size
            if s == 0:
                settle(m, start, size)
            with jax.named_scope(f"gather_{s}_{c}"):
                for item in stage_items(s, z_first, nz, nx, z, x):
                    slot, valid = item[4], item[5]
                    dst = place(m, start, size, slot)
                    if s > 0:
                        arrived(dst, c_recv.at[c, slot], valid)
                    forward(item, z_first, dst, c_send.at[c], c_recv.at[c, slot])
            if 1 < s < stages - 1:
                with jax.named_scope(f"complete_{s}_{c}"):
                    for task in others_first[:each]:
                        complete(*task)
                    others_first = others_first[each:]
        if s == 0:
            with jax.named_scope("late_early"):
                for m in LATE:
                    for j in range(1, nz):
                        e_arrive(m, j)
                for m in range(3):
                    settle(m, 0, spans[m][0])
    with jax.named_scope("drain"):
        for c, (m, h) in enumerate(chunks):
            counts = {}
            for cz in range(nz):
                for cx in range(nx):
                    counts.setdefault(gather_sends(nz, nx, cz, cx, c > 0), []).append(cz * nx + cx)
            for count, places in counts.items():
                here = functools.reduce(jnp.logical_or, [me == at for at in places])
                size = spans[m][1] if m < 2 else spans[m][1] * block // width
                arrived(outs[0].at[pl.ds(0, count * size), :], c_send.at[c], here)
        last = pl.ds(0, n - 1)
        arrived(fg.at[:, last, pl.ds(0, 5 * unit), :], out_sem.at[F_OUT])
        arrived(fg.at[:, last, pl.ds(0, 3 * unit), :], out_sem.at[Y_OUT])
        arrived(fg.at[:, last, pl.ds(0, block // 2), :], out_sem.at[P_OUT])
        arrived(xf.at[:, :, mine, :], out_sem.at[XF_OUT])
        arrived(part.at[:, pl.ds(0, nz * (nx - 1))], out_sem.at[RX_OUT])
        arrived(rz, out_sem.at[RZ_OUT])
        arrived(dg.at[:, last], out_sem.at[D_OUT])
        arrived(st.at[pl.ds(1, tp - 1)], out_sem.at[ST_OUT])
        arrived(sf.at[pl.ds(1, n - 1)], out_sem.at[SF_OUT])
        for m in range(3):
            arrived(early[m].at[last], e_send.at[m])


def store_kernel(*refs):
    count = (len(refs) - 1) // 2
    sems = refs[-1]
    copies = [pltpu.make_async_copy(refs[i], refs[count + i], sems.at[i]) for i in range(count)]
    for copy in copies:
        copy.start()
    for copy in copies:
        copy.wait()


def shards(nz, nx, tp, *args):
    inputs, value_cot, gate_cot, out_cot, conv_output, factors, vw, gw, ow, m1, m2 = args
    n = nz * nx
    block, rank = factors.shape[1], factors.shape[2]
    rows, width = m1.shape[1], m1.shape[2]
    tokens = inputs.shape[0]
    features = inputs.shape[1]
    any_ = pl.BlockSpec(memory_space=pl.ANY)
    vmem = pl.BlockSpec(memory_space=pltpu.VMEM)
    dma = pltpu.SemaphoreType.DMA
    own = tokens // 2
    scratch = [
        pltpu.VMEM((own, features), BF16),
        pltpu.VMEM((own, features), BF16),
        pltpu.VMEM((3, tokens, width), BF16),
        pltpu.VMEM((3, n, block, rank), BF16),
        (pltpu.VMEM(vw.shape, F32), pltpu.VMEM(gw.shape, F32), pltpu.VMEM(ow.shape, F32)),
        pltpu.VMEM((3, own, rank), F32),
        pltpu.VMEM((3, 2, tokens, rank), BF16),
        pltpu.VMEM((3, n, rows, width), F32),
        pltpu.VMEM((3, nx - 1, nz, rows, width), F32),
        pltpu.VMEM((3, nz - 1, rows, width), F32),
        pltpu.VMEM((3, nz, rows, width), F32),
        pltpu.VMEM((3, n, rows, width), BF16),
        pltpu.VMEM((3, rank, width), BF16),
        pltpu.VMEM((3, rank, width), BF16),
        pltpu.VMEM((tp, 8, 128), F32),
        pltpu.VMEM((n, 8, 128), F32),
        (
            pltpu.VMEM((n, block // EARLY, width), BF16),
            pltpu.VMEM((n, block // EARLY, width), BF16),
            pltpu.VMEM((n, width // EARLY, block), BF16),
        ),
        dma((9,)),
        dma((3, n)), dma((3, n)), dma((3, n)), dma((3,)),
        dma((3, nx - 1, nz)), dma((3, nz - 1)), dma((3, n)), dma((2,)), dma((6, n)),
        dma((9,)), dma((6,)), dma((3, n)), dma((3,)),
    ]
    shape = [
        (m1.shape, F32), (m2.shape, F32), (vw.shape, F32), (gw.shape, F32), (ow.shape, F32),
        ((features, width), BF16), ((features, width), BF16), ((width, features), BF16),
    ]
    held = pl.pallas_call(
        functools.partial(kernel, nz, nx, tp, schedule(nz, nx)),
        out_shape=tuple(pltpu.VMEM(*item) for item in shape),
        in_specs=[any_] * 9 + [vmem] * 2,
        out_specs=(vmem,) * 8,
        scratch_shapes=scratch,
        compiler_params=pltpu.CompilerParams(
            collective_id=0, has_side_effects=True, vmem_limit_bytes=VMEM_BYTES
        ),
    )(inputs, out_cot, value_cot, gate_cot, conv_output, factors, vw, gw, ow, m1, m2)
    return pl.pallas_call(
        store_kernel,
        out_shape=tuple(jax.ShapeDtypeStruct(*item) for item in shape),
        in_specs=[vmem] * 8,
        out_specs=(any_,) * 8,
        scratch_shapes=[dma((8,))],
        compiler_params=pltpu.CompilerParams(vmem_limit_bytes=1024 * 1024),
    )(*held)


def solution(mesh):
    fs, tp = mesh.shape["fs"], mesh.shape["tp"]
    nz = 1 << (fs.bit_length() // 2)
    nx = fs // nz
    placed = (
        P("fs", None),
        P("fs", "tp"),
        P("fs", "tp"),
        P("fs", None),
        P("fs", "tp"),
        P(None, "fs", None),
        P("fs", "tp"),
        P("fs", "tp"),
        P("tp", "fs"),
        P(None, "fs", "tp"),
        P(None, "fs", "tp"),
    )
    return jax.shard_map(
        functools.partial(shards, nz, nx, tp),
        mesh=mesh,
        in_specs=placed,
        out_specs=(
            P(None, "fs", "tp"),
            P(None, "fs", "tp"),
            P("fs", "tp"),
            P("fs", "tp"),
            P("tp", "fs"),
            P(None, "tp"),
            P(None, "tp"),
            P("tp", None),
        ),
        check_vma=False,
    )
```

```python
import functools

import jax
import jax.numpy as jnp
from jax import lax
from jax.experimental import pallas as pl
from jax.experimental.pallas import tpu as pltpu
from jax.sharding import PartitionSpec as P

FIRST_DECAY = 0.9
SECOND_DECAY = 0.95
DIVISOR_EPS = 1e-08
SQUARE_EPS = 1e-06
LEARN_RATE = 0.01
K_STEP = 7.0
USE_LAG = 6.5
DIRECTION_GAIN = 128.0
WEIGHT_GAIN = 65536.0
EARLY = 3
EARLY_OF = 16
CUTS = (18, 14, 14)
PARTIAL = (24.0, 28.0, 36.0)
ALONG_Z = (28.6, 36.5, 42.5)
ALONG_STEP = (1.0, 0.3, 1.0)
MOMENTS = (38.0, 47.5, 51.0)
EARLY_Z = (16.0, 20.0, 51.05)
EARLY_HOP = ((21.5, 25.8, 30.0), (25.9, 30.1, 38.6), (55.3, 58.75))
EARLY_X = (39.0, 41.0, None)
OWN_X = (4.5, 9.5, 16.5)
FS_SHARE = 5
GATHER_D = (48.0, 51.1, 54.5)
LAST_D = (52.0, 55.5, 57.5)
VMEM_BYTES = 45 * 1024 * 1024
MESH = pl.DeviceIdType.MESH
F32 = jnp.float32
BF16 = jnp.bfloat16


def high_low(values):
    upper = values.astype(BF16)
    lower = (values - upper.astype(F32)).astype(BF16)
    return upper, lower


def others(coord, size, dist):
    if dist == 0:
        return [(coord, 0, None)]
    if size == 2:
        return [(1 - coord, None, None)]
    return [(coord - dist, -1, coord >= dist), (coord + dist, 1, coord + dist < size)]


def both(*preds):
    preds = [p for p in preds if p is not None]
    if not preds:
        return None
    return functools.reduce(jnp.logical_and, preds)


def run_if(pred, fn):
    if pred is None:
        fn()
    else:
        pl.when(pred)(fn)


def power(values):
    cube = values * values * values
    return cube * cube * cube


def encode(values, gain):
    return power(values * gain).astype(BF16)


def decode(coded, gain):
    value = coded.astype(F32)
    size = jnp.exp(jnp.log(jnp.abs(value)) * (1.0 / 9.0)) * (1.0 / gain)
    return jnp.where(value < 0.0, -size, size)


def stage_items(s, z_first, nz, nx, z, x):
    n1, n2 = (nz, nx) if z_first else (nx, nz)
    c1, c2 = (z, x) if z_first else (x, z)
    items = []
    for e in range(0, n2):
        d = s - e
        if d < 0 or d >= n1:
            continue
        for o1, s1, v1 in others(c1, n1, d):
            for o2, s2, v2 in others(c2, n2, e):
                slot = o1 * nx + o2 if z_first else o2 * nx + o1
                items.append((d, e, s1, s2, slot, both(v1, v2)))
    return items


def gather_sends(nz, nx, z, x, z_first):
    n1, n2 = (nz, nx) if z_first else (nx, nz)
    c1, c2 = (z, x) if z_first else (x, z)
    count = 0
    for o1 in range(n1):
        for o2 in range(n2):
            if o2 == c2:
                count += (o1 <= c1 < n1 - 1) + (o1 >= c1 > 0)
            count += (o2 <= c2 < n2 - 1) + (o2 >= c2 > 0)
    return count


def schedule(nz, nx):
    steps = []

    def add(at, name, *args):
        steps.append((at, name, args))

    def pieces(name, k, first, apart, behind, last):
        for e in range(nx):
            for j in range(nz):
                if j and not e:
                    add(first + apart * (j - 1), name, k, j, e)
                elif e:
                    add(behind if j == 0 else last + 0.4 * j, name, k, j, e)

    for k in range(3):
        at = K_STEP * k
        add(0.01 * k, "f_own_x", k)
        add(5.0 * k, "f_own_z", k)
        add(2.5 + at, "own_part", k)
        for e in range(nx):
            for j in range(nz):
                if j or e:
                    if j == 0:
                        there = 4.0 + 1.8 * k
                    else:
                        there = at + (5.0, 7.0, 9.0)[j - 1] + (4.0 if e else 0.0)
                    if j == nz - 1 and not e:
                        add(there - 1.9, "f_inner", k)
                        add(there, "f_outer", k)
                    else:
                        add(there, "f_arrive", k, j, e)
                    add(there + 3.2, "f_pass", k, j, e)
                    add(max(there + USE_LAG, at + 6.0), "f_use", k, j, e)
        add(at + 13.3 + USE_LAG, "split", k)
        add(PARTIAL[k], "partial", k)
        for step, i in enumerate(list(range(1, nz)) + [0]):
            add(ALONG_Z[k] + ALONG_STEP[k] * step, "along_z", k, i)
        add(MOMENTS[k], "moments", k)
        pieces("d_arrive", k, GATHER_D[k], 0.3, GATHER_D[k] + 0.1, LAST_D[k])
        add(LAST_D[k] + 2.0, "unscaled", k)
    add(MOMENTS[2] + 1.5, "norm")
    for m in range(3):
        add(3.0, "e_code", m)
        add(EARLY_Z[m], "e_own_z", m)
        add(OWN_X[m], "e_own_x", m)
        for d, hop_at in enumerate(EARLY_HOP[m]):
            add(hop_at, "e_hop", m, d + 1)
        if EARLY_X[m] is not None:
            add(EARLY_X[m], "e_cross", m)
    steps.sort(key=lambda step: step[0])
    return steps


def kernel(
    nz, nx, tp, steps_of,
    x_hbm, oc_hbm, vc_hbm, gc_hbm, co_hbm, f_hbm, w0_hbm, w1_hbm, w2_hbm, m1_ref, m2_ref,
    nf_ref, ns_ref, u0_ref, u1_ref, u2_ref, c0_ref, c1_ref, c2_ref,
    x_v, oc_v, cots, fg, wts, acc, xf, part, rx, rz, q, dg, dh, dl, st, sf, early,
    in_sem, f_recv, y_recv, p_recv, xf_recv, rx_recv, rz_recv, d_recv, s_recv, c_recv, out_sem, c_send, e_recv, e_send,
):
    me = lax.axis_index("fs")
    t = lax.axis_index("tp")
    z = lax.div(me, nx)
    x = lax.rem(me, nx)
    n = nz * nx
    core = lax.rem(t, 2)
    row = lax.rem(lax.div(t, 2), 2)
    mate = t + 1 - 2 * core
    beside = t + 2 - 4 * row
    block = f_hbm.shape[1]
    rank = f_hbm.shape[2]
    rows = m1_ref.shape[1]
    width = m1_ref.shape[2]
    own = x_v.shape[0]
    F_OUT, Y_OUT, P_OUT, XF_OUT, RX_OUT, RZ_OUT, D_OUT, ST_OUT, SF_OUT = range(9)

    def remote(src, dst, ssem, rsem, where):
        copy = pltpu.make_async_remote_copy(
            src_ref=src, dst_ref=dst, send_sem=ssem, recv_sem=rsem,
            device_id=where, device_id_type=MESH,
        )
        return copy

    def push(src, group, rsem, where, dst=None):
        remote(src, src if dst is None else dst, out_sem.at[group], rsem, where).start()

    def send(src, ssem, rsem, where, pred, outer):
        run_if(both(pred, outer), remote(src, src, ssem, rsem, where).start)

    def arrived(dst, sem, pred=None):
        run_if(pred, pltpu.make_async_copy(dst, dst, sem).wait)

    mine = pl.ds(pl.multiple_of(core * own, own), own)
    theirs = pl.ds(pl.multiple_of((1 - core) * own, own), own)
    loads = [
        pltpu.make_async_copy(f_hbm, fg.at[:, me], in_sem.at[0]),
        pltpu.make_async_copy(x_hbm.at[mine], x_v, in_sem.at[1]),
        pltpu.make_async_copy(oc_hbm.at[mine], oc_v, in_sem.at[2]),
        pltpu.make_async_copy(vc_hbm, cots.at[0], in_sem.at[3]),
        pltpu.make_async_copy(gc_hbm, cots.at[1], in_sem.at[4]),
        pltpu.make_async_copy(co_hbm, cots.at[2], in_sem.at[5]),
        pltpu.make_async_copy(w0_hbm, wts[0], in_sem.at[6]),
        pltpu.make_async_copy(w1_hbm, wts[1], in_sem.at[7]),
        pltpu.make_async_copy(w2_hbm, wts[2], in_sem.at[8]),
    ]
    for load in loads:
        load.start()

    barrier = pltpu.get_barrier_semaphore()
    everyone = [{"fs": lax.rem(me + k, n)} for k in range(1, n)]
    everyone += [{"tp": lax.rem(t + k, tp)} for k in range(1, tp)]
    for peer in everyone:
        pl.semaphore_signal(barrier, inc=1, device_id=peer, device_id_type=MESH)
    with jax.named_scope("barrier"):
        pl.semaphore_wait(barrier, len(everyone))

    def ranked(j):
        near = [sorted((abs(i - c), i) for i in range(nz))[j][1] for c in range(nz)]
        peer = near[0]
        for c in range(1, nz):
            peer = jnp.where(z == c, near[c], peer)
        return peer

    zs = [ranked(j) for j in range(nz)]
    xs = [lax.rem(x + e, nx) for e in range(nx)]

    def slot_of(j, e):
        return zs[j] * nx + xs[e] if j or e else me

    unit = block // 16
    half = core * (block // 2)
    fs_start = pl.multiple_of(half + row * (8 - FS_SHARE) * unit, unit)
    y_send_start = pl.multiple_of(half + row * FS_SHARE * unit, unit)
    y_recv_start = pl.multiple_of(half + (1 - row) * FS_SHARE * unit, unit)
    mate_half = pl.multiple_of((1 - core) * (block // 2), block // 2)

    def f_part(k, slot, start, size):
        return fg.at[k, slot, pl.ds(start, size), :]

    sources = (x_v, x_v, oc_v)
    spans = [(wide * EARLY // EARLY_OF, wide - wide * EARLY // EARLY_OF) for wide in (block, block, width)]

    def e_push(m, slot, where):
        piece = early[m].at[slot]
        remote(piece, piece, e_send.at[m], e_recv.at[m, slot], {"fs": where}).start()

    def e_code(m):
        loads[6 + m].wait()
        early[m][me] = encode(wts[m][pl.ds(0, spans[m][0]), :], WEIGHT_GAIN)

    def e_own_z(m):
        run_if(z < nz - 1, lambda: e_push(m, me, me + nx))
        run_if(z > 0, lambda: e_push(m, me, me - nx))

    def e_hop(m, d):
        for up, peer in ((1, z - d), (-1, z + d)):
            slot = peer * nx + x

            def relay(up=up, slot=slot):
                arrived(early[m].at[slot], e_recv.at[m, slot])
                onward = z + up
                run_if(jnp.logical_and(onward >= 0, onward < nz), lambda: e_push(m, slot, me + up * nx))

            run_if(jnp.logical_and(peer >= 0, peer < nz), relay)

    def e_own_x(m):
        for e in range(1, nx):
            e_push(m, me, slot_of(0, e))

    def e_cross(m):
        for j in range(1, nz):
            for e in range(1, nx):
                e_push(m, slot_of(j, 0), slot_of(0, e))

    def matmul(k, slot, first):
        cols = pl.ds(pl.multiple_of(slot * block, block), block)
        tile = 256

        def body(i, carry):
            r = pl.ds(pl.multiple_of(i * tile, tile), tile)
            prod = jnp.dot(sources[k][r, cols], fg[k, slot], preferred_element_type=F32)
            if first:
                acc[k, r, :] = prod
            else:
                acc[k, r, :] += prod
            return carry

        lax.fori_loop(0, own // tile, body, 0)

    relayed = nz == 4
    inner = jnp.logical_and(z > 0, z < nz - 1)
    outer = jnp.logical_not(inner)

    def f_own_z(k):
        piece = f_part(k, me, fs_start, FS_SHARE * unit)
        for j in range(1, nz):
            copy = remote(piece, piece, out_sem.at[F_OUT], f_recv.at[k, me], {"fs": slot_of(j, 0)})
            run_if(inner if relayed and j == nz - 1 else None, copy.start)

    def f_inner(k):
        def relay():
            f_arrive(k, nz - 1, 0)
            slot = slot_of(nz - 1, 0)
            end = (z - 1) * (nz - 1)
            push(f_part(k, slot, fs_start, FS_SHARE * unit), F_OUT, f_recv.at[k, slot], {"fs": end * nx + x})

        if relayed:
            run_if(inner, relay)

    def f_outer(k):
        run_if(outer if relayed else None, lambda: f_arrive(k, nz - 1, 0))

    def f_own_x(k):
        piece = f_part(k, me, fs_start, FS_SHARE * unit)
        for e in range(1, nx):
            push(piece, F_OUT, f_recv.at[k, me], {"fs": slot_of(0, e)})

    def f_arrive(k, j, e):
        slot = slot_of(j, e)
        piece = f_part(k, slot, fs_start, FS_SHARE * unit)
        arrived(piece, f_recv.at[k, slot])
        if e == 0:
            for other in range(1, nx):
                push(piece, F_OUT, f_recv.at[k, slot], {"fs": slot_of(0, other)})
        push(f_part(k, slot, y_send_start, (8 - FS_SHARE) * unit), Y_OUT, y_recv.at[k, slot], {"tp": beside})
        push(piece, P_OUT, p_recv.at[k, slot], {"tp": mate})

    def f_pass(k, j, e):
        slot = slot_of(j, e)
        piece = f_part(k, slot, y_recv_start, (8 - FS_SHARE) * unit)
        arrived(piece, y_recv.at[k, slot])
        push(piece, P_OUT, p_recv.at[k, slot], {"tp": mate})

    def f_use(k, j, e):
        slot = slot_of(j, e)
        arrived(f_part(k, slot, mate_half, block // 2), p_recv.at[k, slot])
        matmul(k, slot, False)

    def own_part(k):
        if k != 1:
            loads[1 + k // 2].wait()
        matmul(k, me, True)

    dims = (((0,), (0,)), ((), ()))

    def product(k, r):
        prod = lax.dot_general(xf[k, 0, r, :], cots[k, r, :], dims, preferred_element_type=F32)
        prod = prod + lax.dot_general(xf[k, 1, r, :], cots[k, r, :], dims, preferred_element_type=F32)
        return prod.reshape(n, rows, width)

    def split(k):
        upper, lower = high_low(acc[k])
        xf[k, 0, mine, :] = upper
        xf[k, 1, mine, :] = lower
        push(xf.at[k, :, mine, :], XF_OUT, xf_recv.at[k], {"tp": mate})
        loads[3 + k].wait()
        part[k] = product(k, mine)

    order = list(range(1, nz)) + [0]

    def partial(k):
        arrived(xf.at[k, :, theirs, :], xf_recv.at[k])
        part[k] = part[k] + product(k, theirs)
        for i in order:
            oz = lax.rem(z + i, nz)
            for e in range(1, nx):
                slot = oz * nx + xs[e]
                push(part.at[k, slot], RX_OUT, rx_recv.at[k, e - 1, i], {"fs": z * nx + xs[e]}, rx.at[k, e - 1, i])

    def along_z(k, i):
        oz = lax.rem(z + i, nz)
        value = part[k, oz * nx + x]
        for e in range(1, nx):
            arrived(rx.at[k, e - 1, i], rx_recv.at[k, e - 1, i])
            value = value + rx[k, e - 1, i]
        q[k, i] = value
        if i:
            push(q.at[k, i], RZ_OUT, rz_recv.at[k, i - 1], {"fs": oz * nx + x}, rz.at[k, i - 1])

    def moments(k):
        projected = q[k, 0]
        for i in range(1, nz):
            arrived(rz.at[k, i - 1], rz_recv.at[k, i - 1])
            projected = projected + rz[k, i - 1]
        new_first = FIRST_DECAY * m1_ref[k] + (1.0 - FIRST_DECAY) * projected
        new_second = SECOND_DECAY * m2_ref[k] + (1.0 - SECOND_DECAY) * projected * projected
        nf_ref[k] = new_first
        ns_ref[k] = new_second
        direction = new_first / (jnp.sqrt(new_second) + DIVISOR_EPS)
        dg[k, me] = encode(direction, DIRECTION_GAIN)
        piece = dg.at[k, me]
        for j in range(nz - 1, 0, -1):
            push(piece, D_OUT, d_recv.at[k, me], {"fs": slot_of(j, 0)})
        for e in range(1, nx):
            push(piece, D_OUT, d_recv.at[k, me], {"fs": slot_of(0, e)})
        square = jnp.sum((direction * direction).reshape(rows * width // 1024, 8, 128), axis=0)
        st[0] = square if k == 0 else st[0] + square
        if k == 2:
            for i in range(1, tp):
                push(st.at[0], ST_OUT, s_recv.at[0], {"tp": lax.rem(t + i, tp)}, st.at[tp - i])

    def norm():
        arrived(st.at[pl.ds(1, tp - 1)], s_recv.at[0])
        value = st[0]
        for i in range(1, tp):
            value = value + st[i]
        sf[0] = value
        for i in range(1, n):
            push(sf.at[0], SF_OUT, s_recv.at[1], {"fs": lax.rem(me + i, n)}, sf.at[n - i])

    def d_arrive(k, j, e):
        slot = slot_of(j, e)
        piece = dg.at[k, slot]
        arrived(piece, d_recv.at[k, slot])
        if e == 0:
            for other in range(1, nx):
                push(piece, D_OUT, d_recv.at[k, slot], {"fs": slot_of(0, other)})

    tdims = (((0,), (1,)), ((), ()))
    news = (u0_ref, u1_ref, u2_ref)

    def unscaled(k):
        value = decode(dg[k].reshape(rank, width), DIRECTION_GAIN)
        upper, lower = high_low(value)
        dh[k] = upper
        dl[k] = lower
        if k < 2:
            news[k][...] = jnp.dot(fg[k, me], dh[k], preferred_element_type=F32) + jnp.dot(
                fg[k, me], dl[k], preferred_element_type=F32
            )
        else:
            news[k][...] = lax.dot_general(dh[k], fg[k, me], tdims, preferred_element_type=F32) + lax.dot_general(
                dl[k], fg[k, me], tdims, preferred_element_type=F32
            )

    table = dict(
        f_own_z=f_own_z, f_own_x=f_own_x, f_arrive=f_arrive, f_pass=f_pass, f_use=f_use, own_part=own_part,
        split=split, partial=partial, along_z=along_z, moments=moments, d_arrive=d_arrive, norm=norm,
        unscaled=unscaled, e_code=e_code, e_own_z=e_own_z, e_own_x=e_own_x, e_hop=e_hop, e_cross=e_cross, f_inner=f_inner, f_outer=f_outer,
    )
    loads[0].wait()
    for _, name, args in steps_of:
        with jax.named_scope(name + "_" + "_".join(str(v) for v in args)):
            table[name](*args)

    with jax.named_scope("total"):
        arrived(sf.at[pl.ds(1, n - 1)], s_recv.at[1])
        sums = sf[0]
        for i in range(1, n):
            sums = sums + sf[i]
        total = jnp.sum(jnp.sum(sums, axis=0, keepdims=True), axis=1, keepdims=True)
        scale = lax.rsqrt(total / (3 * rank * width * tp) + SQUARE_EPS)

    outs = (c0_ref, c1_ref, c2_ref)
    chunks = [(m, h) for m in range(3) for h in range(2)]
    others_first = [(m, j, e) for e in range(nx) for j in range(nz) if j or e for m in range(3)]

    def chunk_span(m, h):
        first, rest = spans[m]
        cut = rest * CUTS[m] // 28 // 16 * 16
        return (first + cut, rest - cut) if h else (first, cut)

    def place(m, start, size, slot):
        if m < 2:
            return outs[m].at[pl.ds(pl.multiple_of(slot * block + start, 16), size), :]
        return outs[m].at[pl.ds(start, size), pl.ds(pl.multiple_of(slot * block, block), block)]

    def settle(m, start, size):
        r = pl.ds(start, size)
        update = scale * news[m][r, :]
        news[m][r, :] = update
        place(m, start, size, me)[...] = (wts[m][r, :] - LEARN_RATE * update).astype(BF16)

    def complete(m, j, e):
        slot = slot_of(j, e)
        first = spans[m][0]
        if e:
            arrived(early[m].at[slot], e_recv.at[m, slot])
        if m < 2:
            rows_in = fg[m, slot, pl.ds(0, first), :]
            update = jnp.dot(rows_in, dh[m], preferred_element_type=F32)
            update = update + jnp.dot(rows_in, dl[m], preferred_element_type=F32)
        else:
            cols = pl.ds(0, first)
            update = lax.dot_general(dh[2, :, cols], fg[2, slot], tdims, preferred_element_type=F32)
            update = update + lax.dot_general(dl[2, :, cols], fg[2, slot], tdims, preferred_element_type=F32)
        weight = decode(early[m][slot], WEIGHT_GAIN)
        place(m, 0, first, slot)[...] = (weight - LEARN_RATE * (scale * update)).astype(BF16)

    def forward(item, z_first, src, ssem, rsem):
        d, e, s1, s2, slot, valid = item
        n1, n2 = (nz, nx) if z_first else (nx, nz)
        c1, c2 = (z, x) if z_first else (x, z)
        st1, st2 = (nx, 1) if z_first else (1, nx)
        if e == 0 and d < n1 - 1:
            if s1 in (-1, 0):
                send(src, ssem, rsem, {"fs": me + st1}, c1 + 1 < n1, valid)
            if s1 in (1, 0):
                send(src, ssem, rsem, {"fs": me - st1}, c1 > 0, valid)
        if e < n2 - 1:
            if s2 in (-1, 0):
                send(src, ssem, rsem, {"fs": me + st2}, c2 + 1 < n2, valid)
            if s2 in (1, 0):
                send(src, ssem, rsem, {"fs": me - st2}, c2 > 0, valid)

    stages = nz + nx - 1
    last_waits = []
    each = -(-len(others_first) // (len(chunks) * (stages - 3)))
    for s in range(stages):
        for c, (m, h) in enumerate(chunks):
            z_first = c > 0
            start, size = chunk_span(m, h)
            if s == 0:
                settle(m, start, size)
            with jax.named_scope(f"gather_{s}_{c}"):
                for item in stage_items(s, z_first, nz, nx, z, x):
                    slot, valid = item[4], item[5]
                    dst = place(m, start, size, slot)
                    if item[1] == (nx if z_first else nz) - 1:
                        last_waits.append((dst, c_recv.at[c, slot], valid))
                        continue
                    if s > 0:
                        arrived(dst, c_recv.at[c, slot], valid)
                    forward(item, z_first, dst, c_send.at[c], c_recv.at[c, slot])
            if 1 < s < stages - 1:
                with jax.named_scope(f"complete_{s}_{c}"):
                    for task in others_first[:each]:
                        complete(*task)
                    others_first = others_first[each:]
        if s == 0:
            with jax.named_scope("late_early"):
                for late in range(3):
                    for d in range(len(EARLY_HOP[late]) + 1, nz):
                        e_hop(late, d)
                    if EARLY_X[late] is None:
                        e_cross(late)
                for m in range(3):
                    settle(m, 0, spans[m][0])
    with jax.named_scope("last_waits"):
        for dst, sem, valid in last_waits:
            arrived(dst, sem, valid)
    with jax.named_scope("drain"):
        for c, (m, h) in enumerate(chunks):
            counts = {}
            for cz in range(nz):
                for cx in range(nx):
                    counts.setdefault(gather_sends(nz, nx, cz, cx, c > 0), []).append(cz * nx + cx)
            for count, places in counts.items():
                here = functools.reduce(jnp.logical_or, [me == at for at in places])
                size = chunk_span(m, h)[1]
                size = size if m < 2 else size * block // width
                arrived(outs[0].at[pl.ds(0, count * size), :], c_send.at[c], here)
        last = pl.ds(0, n - 1)
        if relayed:
            arrived(fg.at[:, pl.ds(0, n - 2), pl.ds(0, FS_SHARE * unit), :], out_sem.at[F_OUT], outer)
            arrived(fg.at[:, pl.ds(0, n), pl.ds(0, FS_SHARE * unit), :], out_sem.at[F_OUT], inner)
        else:
            arrived(fg.at[:, last, pl.ds(0, FS_SHARE * unit), :], out_sem.at[F_OUT])
        arrived(fg.at[:, last, pl.ds(0, (8 - FS_SHARE) * unit), :], out_sem.at[Y_OUT])
        arrived(fg.at[:, last, pl.ds(0, block // 2), :], out_sem.at[P_OUT])
        arrived(xf.at[:, :, mine, :], out_sem.at[XF_OUT])
        arrived(part.at[:, pl.ds(0, nz * (nx - 1))], out_sem.at[RX_OUT])
        arrived(rz, out_sem.at[RZ_OUT])
        arrived(dg.at[:, last], out_sem.at[D_OUT])
        arrived(st.at[pl.ds(1, tp - 1)], out_sem.at[ST_OUT])
        arrived(sf.at[pl.ds(1, n - 1)], out_sem.at[SF_OUT])
        for m in range(3):
            size = spans[m][0] if m < 2 else spans[m][0] * block // width
            counts = {}
            for cz in range(nz):
                count = nz * (nx - 1) + (cz < nz - 1) * (cz + 1) + (cz > 0) * (nz - cz)
                counts.setdefault(count, []).append(cz)
            for count, places in counts.items():
                here = functools.reduce(jnp.logical_or, [z == at for at in places])
                arrived(outs[0].at[pl.ds(0, count * size), :], e_send.at[m], here)


def store_kernel(*refs):
    count = (len(refs) - 1) // 2
    sems = refs[-1]
    copies = [pltpu.make_async_copy(refs[i], refs[count + i], sems.at[i]) for i in range(count)]
    for copy in copies:
        copy.start()
    for copy in copies:
        copy.wait()


def shards(nz, nx, tp, *args):
    inputs, value_cot, gate_cot, out_cot, conv_output, factors, vw, gw, ow, m1, m2 = args
    n = nz * nx
    block, rank = factors.shape[1], factors.shape[2]
    rows, width = m1.shape[1], m1.shape[2]
    tokens = inputs.shape[0]
    features = inputs.shape[1]
    any_ = pl.BlockSpec(memory_space=pl.ANY)
    vmem = pl.BlockSpec(memory_space=pltpu.VMEM)
    dma = pltpu.SemaphoreType.DMA
    own = tokens // 2
    scratch = [
        pltpu.VMEM((own, features), BF16),
        pltpu.VMEM((own, features), BF16),
        pltpu.VMEM((3, tokens, width), BF16),
        pltpu.VMEM((3, n, block, rank), BF16),
        (pltpu.VMEM(vw.shape, F32), pltpu.VMEM(gw.shape, F32), pltpu.VMEM(ow.shape, F32)),
        pltpu.VMEM((3, own, rank), F32),
        pltpu.VMEM((3, 2, tokens, rank), BF16),
        pltpu.VMEM((3, n, rows, width), F32),
        pltpu.VMEM((3, nx - 1, nz, rows, width), F32),
        pltpu.VMEM((3, nz - 1, rows, width), F32),
        pltpu.VMEM((3, nz, rows, width), F32),
        pltpu.VMEM((3, n, rows, width), BF16),
        pltpu.VMEM((3, rank, width), BF16),
        pltpu.VMEM((3, rank, width), BF16),
        pltpu.VMEM((tp, 8, 128), F32),
        pltpu.VMEM((n, 8, 128), F32),
        (
            pltpu.VMEM((n, block * EARLY // EARLY_OF, width), BF16),
            pltpu.VMEM((n, block * EARLY // EARLY_OF, width), BF16),
            pltpu.VMEM((n, width * EARLY // EARLY_OF, block), BF16),
        ),
        dma((9,)),
        dma((3, n)), dma((3, n)), dma((3, n)), dma((3,)),
        dma((3, nx - 1, nz)), dma((3, nz - 1)), dma((3, n)), dma((2,)), dma((6, n)),
        dma((9,)), dma((6,)), dma((3, n)), dma((3,)),
    ]
    shape = [
        (m1.shape, F32), (m2.shape, F32), (vw.shape, F32), (gw.shape, F32), (ow.shape, F32),
        ((features, width), BF16), ((features, width), BF16), ((width, features), BF16),
    ]
    held = pl.pallas_call(
        functools.partial(kernel, nz, nx, tp, schedule(nz, nx)),
        out_shape=tuple(pltpu.VMEM(*item) for item in shape),
        in_specs=[any_] * 9 + [vmem] * 2,
        out_specs=(vmem,) * 8,
        scratch_shapes=scratch,
        compiler_params=pltpu.CompilerParams(
            collective_id=0, has_side_effects=True, vmem_limit_bytes=VMEM_BYTES
        ),
    )(inputs, out_cot, value_cot, gate_cot, conv_output, factors, vw, gw, ow, m1, m2)
    return pl.pallas_call(
        store_kernel,
        out_shape=tuple(jax.ShapeDtypeStruct(*item) for item in shape),
        in_specs=[vmem] * 8,
        out_specs=(any_,) * 8,
        scratch_shapes=[dma((8,))],
        compiler_params=pltpu.CompilerParams(vmem_limit_bytes=1024 * 1024),
    )(*held)


def solution(mesh):
    fs, tp = mesh.shape["fs"], mesh.shape["tp"]
    nz = 1 << (fs.bit_length() // 2)
    nx = fs // nz
    placed = (
        P("fs", None),
        P("fs", "tp"),
        P("fs", "tp"),
        P("fs", None),
        P("fs", "tp"),
        P(None, "fs", None),
        P("fs", "tp"),
        P("fs", "tp"),
        P("tp", "fs"),
        P(None, "fs", "tp"),
        P(None, "fs", "tp"),
    )
    return jax.shard_map(
        functools.partial(shards, nz, nx, tp),
        mesh=mesh,
        in_specs=placed,
        out_specs=(
            P(None, "fs", "tp"),
            P(None, "fs", "tp"),
            P("fs", "tp"),
            P("fs", "tp"),
            P("tp", "fs"),
            P(None, "tp"),
            P(None, "tp"),
            P("tp", None),
        ),
        check_vma=False,
    )
```

```python
import functools

import jax
import jax.numpy as jnp
from jax import lax
from jax.experimental import pallas as pl
from jax.experimental.pallas import tpu as pltpu
from jax.sharding import PartitionSpec as P

FIRST_DECAY = 0.9
SECOND_DECAY = 0.95
DIVISOR_EPS = 1e-08
SQUARE_EPS = 1e-06
LEARN_RATE = 0.01
K_STEP = 7.0
USE_LAG = 5.5
DIRECTION_GAIN = 128.0
WEIGHT_GAIN = 65536.0
EARLY = 3
EARLY_OF = 16
CUTS = (18, 14, 14)
PARTIAL = (24.0, 28.0, 36.0)
ALONG_Z = (28.6, 36.5, 42.5)
ALONG_STEP = (1.0, 0.3, 1.0)
MOMENTS = (38.0, 47.5, 51.0)
EARLY_Z = (16.0, 20.0, 51.05)
EARLY_HOP = ((21.5, 25.8, 30.0), (25.9, 30.1, 38.6), (55.3, 58.75))
EARLY_X = (39.0, 56.0, None)
OWN_X = (8.5, 12.5, 16.5)
FS_SHARE = 5
CODE_AT = 8.4
CROSS_LAG = 5.0
FINISH = 3
ORDER = (1, 2, 3, 4, 5, 0)
GATHER_D = (48.0, 51.1, 54.5)
LAST_D = (52.0, 55.5, 57.5)
VMEM_BYTES = 45 * 1024 * 1024
MESH = pl.DeviceIdType.MESH
F32 = jnp.float32
BF16 = jnp.bfloat16


def high_low(values):
    upper = values.astype(BF16)
    lower = (values - upper.astype(F32)).astype(BF16)
    return upper, lower


def others(coord, size, dist):
    if dist == 0:
        return [(coord, 0, None)]
    if size == 2:
        return [(1 - coord, None, None)]
    return [(coord - dist, -1, coord >= dist), (coord + dist, 1, coord + dist < size)]


def both(*preds):
    preds = [p for p in preds if p is not None]
    if not preds:
        return None
    return functools.reduce(jnp.logical_and, preds)


def run_if(pred, fn):
    if pred is None:
        fn()
    else:
        pl.when(pred)(fn)


def power(values):
    cube = values * values * values
    return cube * cube * cube


def encode(values, gain):
    return power(values * gain).astype(BF16)


def decode(coded, gain):
    value = coded.astype(F32)
    size = jnp.exp(jnp.log(jnp.abs(value)) * (1.0 / 9.0)) * (1.0 / gain)
    return jnp.where(value < 0.0, -size, size)


def stage_items(s, z_first, nz, nx, z, x):
    n1, n2 = (nz, nx) if z_first else (nx, nz)
    c1, c2 = (z, x) if z_first else (x, z)
    items = []
    for e in range(0, n2):
        d = s - e
        if d < 0 or d >= n1:
            continue
        for o1, s1, v1 in others(c1, n1, d):
            for o2, s2, v2 in others(c2, n2, e):
                slot = o1 * nx + o2 if z_first else o2 * nx + o1
                items.append((d, e, s1, s2, slot, both(v1, v2)))
    return items


def gather_sends(nz, nx, z, x, z_first):
    n1, n2 = (nz, nx) if z_first else (nx, nz)
    c1, c2 = (z, x) if z_first else (x, z)
    count = 0
    for o1 in range(n1):
        for o2 in range(n2):
            if o2 == c2:
                count += (o1 <= c1 < n1 - 1) + (o1 >= c1 > 0)
            count += (o2 <= c2 < n2 - 1) + (o2 >= c2 > 0)
    return count


def schedule(nz, nx):
    steps = []

    def add(at, name, *args):
        steps.append((at, name, args))

    def pieces(name, k, first, apart, behind, last):
        for e in range(nx):
            for j in range(nz):
                if j and not e:
                    add(first + apart * (j - 1), name, k, j, e)
                elif e:
                    add(behind if j == 0 else last + 0.4 * j, name, k, j, e)

    for k in range(3):
        at = K_STEP * k
        add(0.01 * k, "f_own_x", k)
        add(5.0 * k, "f_own_z", k)
        add(2.5 + at, "own_part", k)
        for e in range(nx):
            for j in range(nz):
                if j or e:
                    if j == 0:
                        there = 4.0 + 1.8 * k
                    else:
                        there = at + (5.0, 7.0, 9.0)[j - 1] + (CROSS_LAG if e else 0.0)
                    if j == nz - 1 and not e:
                        add(there - 1.9, "f_inner", k)
                        add(there, "f_outer", k)
                    else:
                        add(there, "f_arrive", k, j, e)
                    add(there + 3.2, "f_pass", k, j, e)
                    add(max(there + USE_LAG, at + 6.0), "f_use", k, j, e)
        add(at + 9.3 + CROSS_LAG + USE_LAG, "split", k)
        add(PARTIAL[k], "partial", k)
        for step, i in enumerate(list(range(1, nz)) + [0]):
            add(ALONG_Z[k] + ALONG_STEP[k] * step, "along_z", k, i)
        add(MOMENTS[k], "moments", k)
        pieces("d_arrive", k, GATHER_D[k], 0.3, GATHER_D[k] + 0.1, LAST_D[k])
        add(LAST_D[k] + 2.0, "unscaled", k)
    add(MOMENTS[2] + 1.5, "norm")
    for m in range(3):
        add(CODE_AT, "e_code", m)
        add(EARLY_Z[m], "e_own_z", m)
        add(OWN_X[m], "e_own_x", m)
        for d, hop_at in enumerate(EARLY_HOP[m]):
            add(hop_at, "e_hop", m, d + 1)
        if EARLY_X[m] is not None:
            add(EARLY_X[m], "e_cross", m)
    steps.sort(key=lambda step: step[0])
    return steps


def kernel(
    nz, nx, tp, steps_of,
    x_hbm, oc_hbm, vc_hbm, gc_hbm, co_hbm, f_hbm, w0_hbm, w1_hbm, w2_hbm, m1_ref, m2_ref,
    nf_ref, ns_ref, u0_ref, u1_ref, u2_ref, c0_ref, c1_ref, c2_ref,
    x_v, oc_v, cots, fg, wts, acc, xf, part, rx, rz, q, dg, dh, dl, st, sf, early,
    in_sem, f_recv, y_recv, p_recv, xf_recv, rx_recv, rz_recv, d_recv, s_recv, c_recv, out_sem, c_send, e_recv, e_send,
):
    me = lax.axis_index("fs")
    t = lax.axis_index("tp")
    z = lax.div(me, nx)
    x = lax.rem(me, nx)
    n = nz * nx
    core = lax.rem(t, 2)
    row = lax.rem(lax.div(t, 2), 2)
    mate = t + 1 - 2 * core
    beside = t + 2 - 4 * row
    block = f_hbm.shape[1]
    rank = f_hbm.shape[2]
    rows = m1_ref.shape[1]
    width = m1_ref.shape[2]
    own = x_v.shape[0]
    F_OUT, Y_OUT, P_OUT, XF_OUT, RX_OUT, RZ_OUT, D_OUT, ST_OUT, SF_OUT = range(9)

    def remote(src, dst, ssem, rsem, where):
        copy = pltpu.make_async_remote_copy(
            src_ref=src, dst_ref=dst, send_sem=ssem, recv_sem=rsem,
            device_id=where, device_id_type=MESH,
        )
        return copy

    def push(src, group, rsem, where, dst=None):
        remote(src, src if dst is None else dst, out_sem.at[group], rsem, where).start()

    def send(src, ssem, rsem, where, pred, outer):
        run_if(both(pred, outer), remote(src, src, ssem, rsem, where).start)

    def arrived(dst, sem, pred=None):
        run_if(pred, pltpu.make_async_copy(dst, dst, sem).wait)

    mine = pl.ds(pl.multiple_of(core * own, own), own)
    theirs = pl.ds(pl.multiple_of((1 - core) * own, own), own)
    loads = [
        pltpu.make_async_copy(f_hbm, fg.at[:, me], in_sem.at[0]),
        pltpu.make_async_copy(x_hbm.at[mine], x_v, in_sem.at[1]),
        pltpu.make_async_copy(oc_hbm.at[mine], oc_v, in_sem.at[2]),
        pltpu.make_async_copy(vc_hbm, cots.at[0], in_sem.at[3]),
        pltpu.make_async_copy(gc_hbm, cots.at[1], in_sem.at[4]),
        pltpu.make_async_copy(co_hbm, cots.at[2], in_sem.at[5]),
        pltpu.make_async_copy(w0_hbm, wts[0], in_sem.at[6]),
        pltpu.make_async_copy(w1_hbm, wts[1], in_sem.at[7]),
        pltpu.make_async_copy(w2_hbm, wts[2], in_sem.at[8]),
    ]
    for load in loads:
        load.start()

    barrier = pltpu.get_barrier_semaphore()
    everyone = [{"fs": lax.rem(me + k, n)} for k in range(1, n)]
    everyone += [{"tp": lax.rem(t + k, tp)} for k in range(1, tp)]
    for peer in everyone:
        pl.semaphore_signal(barrier, inc=1, device_id=peer, device_id_type=MESH)
    with jax.named_scope("barrier"):
        pl.semaphore_wait(barrier, len(everyone))

    def ranked(j):
        near = [sorted((abs(i - c), i) for i in range(nz))[j][1] for c in range(nz)]
        peer = near[0]
        for c in range(1, nz):
            peer = jnp.where(z == c, near[c], peer)
        return peer

    zs = [ranked(j) for j in range(nz)]
    xs = [lax.rem(x + e, nx) for e in range(nx)]

    def slot_of(j, e):
        return zs[j] * nx + xs[e] if j or e else me

    unit = block // 16
    half = core * (block // 2)
    fs_start = pl.multiple_of(half + row * (8 - FS_SHARE) * unit, unit)
    y_send_start = pl.multiple_of(half + row * FS_SHARE * unit, unit)
    y_recv_start = pl.multiple_of(half + (1 - row) * FS_SHARE * unit, unit)
    mate_half = pl.multiple_of((1 - core) * (block // 2), block // 2)

    def f_part(k, slot, start, size):
        return fg.at[k, slot, pl.ds(start, size), :]

    sources = (x_v, x_v, oc_v)
    spans = [(wide * EARLY // EARLY_OF, wide - wide * EARLY // EARLY_OF) for wide in (block, block, width)]

    def e_push(m, slot, where):
        piece = early[m].at[slot]
        remote(piece, piece, e_send.at[m], e_recv.at[m, slot], {"fs": where}).start()

    def e_code(m):
        loads[6 + m].wait()
        early[m][me] = encode(wts[m][pl.ds(0, spans[m][0]), :], WEIGHT_GAIN)

    def e_own_z(m):
        run_if(z < nz - 1, lambda: e_push(m, me, me + nx))
        run_if(z > 0, lambda: e_push(m, me, me - nx))

    def e_hop(m, d):
        for up, peer in ((1, z - d), (-1, z + d)):
            slot = peer * nx + x

            def relay(up=up, slot=slot):
                arrived(early[m].at[slot], e_recv.at[m, slot])
                onward = z + up
                run_if(jnp.logical_and(onward >= 0, onward < nz), lambda: e_push(m, slot, me + up * nx))

            run_if(jnp.logical_and(peer >= 0, peer < nz), relay)

    def e_own_x(m):
        for e in range(1, nx):
            e_push(m, me, slot_of(0, e))

    def e_cross(m):
        for j in range(1, nz):
            for e in range(1, nx):
                e_push(m, slot_of(j, 0), slot_of(0, e))

    def matmul(k, slot, first):
        cols = pl.ds(pl.multiple_of(slot * block, block), block)
        tile = 256

        def body(i, carry):
            r = pl.ds(pl.multiple_of(i * tile, tile), tile)
            prod = jnp.dot(sources[k][r, cols], fg[k, slot], preferred_element_type=F32)
            if first:
                acc[k, r, :] = prod
            else:
                acc[k, r, :] += prod
            return carry

        lax.fori_loop(0, own // tile, body, 0)

    relayed = nz == 4
    inner = jnp.logical_and(z > 0, z < nz - 1)
    outer = jnp.logical_not(inner)

    def f_own_z(k):
        piece = f_part(k, me, fs_start, FS_SHARE * unit)
        for j in range(1, nz):
            copy = remote(piece, piece, out_sem.at[F_OUT], f_recv.at[k, me], {"fs": slot_of(j, 0)})
            run_if(inner if relayed and j == nz - 1 else None, copy.start)

    def f_inner(k):
        def relay():
            f_arrive(k, nz - 1, 0)
            slot = slot_of(nz - 1, 0)
            end = (z - 1) * (nz - 1)
            push(f_part(k, slot, fs_start, FS_SHARE * unit), F_OUT, f_recv.at[k, slot], {"fs": end * nx + x})

        if relayed:
            run_if(inner, relay)

    def f_outer(k):
        run_if(outer if relayed else None, lambda: f_arrive(k, nz - 1, 0))

    def f_own_x(k):
        piece = f_part(k, me, fs_start, FS_SHARE * unit)
        for e in range(1, nx):
            push(piece, F_OUT, f_recv.at[k, me], {"fs": slot_of(0, e)})

    def f_arrive(k, j, e):
        slot = slot_of(j, e)
        piece = f_part(k, slot, fs_start, FS_SHARE * unit)
        arrived(piece, f_recv.at[k, slot])
        if e == 0:
            for other in range(1, nx):
                push(piece, F_OUT, f_recv.at[k, slot], {"fs": slot_of(0, other)})
        push(f_part(k, slot, y_send_start, (8 - FS_SHARE) * unit), Y_OUT, y_recv.at[k, slot], {"tp": beside})
        push(piece, P_OUT, p_recv.at[k, slot], {"tp": mate})

    def f_pass(k, j, e):
        slot = slot_of(j, e)
        piece = f_part(k, slot, y_recv_start, (8 - FS_SHARE) * unit)
        arrived(piece, y_recv.at[k, slot])
        push(piece, P_OUT, p_recv.at[k, slot], {"tp": mate})

    def f_use(k, j, e):
        slot = slot_of(j, e)
        arrived(f_part(k, slot, mate_half, block // 2), p_recv.at[k, slot])
        matmul(k, slot, False)

    def own_part(k):
        if k != 1:
            loads[1 + k // 2].wait()
        matmul(k, me, True)

    dims = (((0,), (0,)), ((), ()))

    def product(k, r):
        prod = lax.dot_general(xf[k, 0, r, :], cots[k, r, :], dims, preferred_element_type=F32)
        prod = prod + lax.dot_general(xf[k, 1, r, :], cots[k, r, :], dims, preferred_element_type=F32)
        return prod.reshape(n, rows, width)

    def split(k):
        upper, lower = high_low(acc[k])
        xf[k, 0, mine, :] = upper
        xf[k, 1, mine, :] = lower
        push(xf.at[k, :, mine, :], XF_OUT, xf_recv.at[k], {"tp": mate})
        loads[3 + k].wait()
        part[k] = product(k, mine)

    order = list(range(1, nz)) + [0]

    def partial(k):
        arrived(xf.at[k, :, theirs, :], xf_recv.at[k])
        part[k] = part[k] + product(k, theirs)
        for i in order:
            oz = lax.rem(z + i, nz)
            for e in range(1, nx):
                slot = oz * nx + xs[e]
                push(part.at[k, slot], RX_OUT, rx_recv.at[k, e - 1, i], {"fs": z * nx + xs[e]}, rx.at[k, e - 1, i])

    def along_z(k, i):
        oz = lax.rem(z + i, nz)
        value = part[k, oz * nx + x]
        for e in range(1, nx):
            arrived(rx.at[k, e - 1, i], rx_recv.at[k, e - 1, i])
            value = value + rx[k, e - 1, i]
        q[k, i] = value
        if i:
            push(q.at[k, i], RZ_OUT, rz_recv.at[k, i - 1], {"fs": oz * nx + x}, rz.at[k, i - 1])

    def moments(k):
        projected = q[k, 0]
        for i in range(1, nz):
            arrived(rz.at[k, i - 1], rz_recv.at[k, i - 1])
            projected = projected + rz[k, i - 1]
        new_first = FIRST_DECAY * m1_ref[k] + (1.0 - FIRST_DECAY) * projected
        new_second = SECOND_DECAY * m2_ref[k] + (1.0 - SECOND_DECAY) * projected * projected
        nf_ref[k] = new_first
        ns_ref[k] = new_second
        direction = new_first / (jnp.sqrt(new_second) + DIVISOR_EPS)
        dg[k, me] = encode(direction, DIRECTION_GAIN)
        piece = dg.at[k, me]
        for j in range(nz - 1, 0, -1):
            push(piece, D_OUT, d_recv.at[k, me], {"fs": slot_of(j, 0)})
        for e in range(1, nx):
            push(piece, D_OUT, d_recv.at[k, me], {"fs": slot_of(0, e)})
        square = jnp.sum((direction * direction).reshape(rows * width // 1024, 8, 128), axis=0)
        st[0] = square if k == 0 else st[0] + square
        if k == 2:
            for i in range(1, tp):
                push(st.at[0], ST_OUT, s_recv.at[0], {"tp": lax.rem(t + i, tp)}, st.at[tp - i])

    def norm():
        arrived(st.at[pl.ds(1, tp - 1)], s_recv.at[0])
        value = st[0]
        for i in range(1, tp):
            value = value + st[i]
        sf[0] = value
        for i in range(1, n):
            push(sf.at[0], SF_OUT, s_recv.at[1], {"fs": lax.rem(me + i, n)}, sf.at[n - i])

    def d_arrive(k, j, e):
        slot = slot_of(j, e)
        piece = dg.at[k, slot]
        arrived(piece, d_recv.at[k, slot])
        if e == 0:
            for other in range(1, nx):
                push(piece, D_OUT, d_recv.at[k, slot], {"fs": slot_of(0, other)})

    tdims = (((0,), (1,)), ((), ()))
    news = (u0_ref, u1_ref, u2_ref)

    def unscaled(k):
        value = decode(dg[k].reshape(rank, width), DIRECTION_GAIN)
        upper, lower = high_low(value)
        dh[k] = upper
        dl[k] = lower
        if k < 2:
            news[k][...] = jnp.dot(fg[k, me], dh[k], preferred_element_type=F32) + jnp.dot(
                fg[k, me], dl[k], preferred_element_type=F32
            )
        else:
            news[k][...] = lax.dot_general(dh[k], fg[k, me], tdims, preferred_element_type=F32) + lax.dot_general(
                dl[k], fg[k, me], tdims, preferred_element_type=F32
            )

    table = dict(
        f_own_z=f_own_z, f_own_x=f_own_x, f_arrive=f_arrive, f_pass=f_pass, f_use=f_use, own_part=own_part,
        split=split, partial=partial, along_z=along_z, moments=moments, d_arrive=d_arrive, norm=norm,
        unscaled=unscaled, e_code=e_code, e_own_z=e_own_z, e_own_x=e_own_x, e_hop=e_hop, e_cross=e_cross, f_inner=f_inner, f_outer=f_outer,
    )
    loads[0].wait()
    for _, name, args in steps_of:
        with jax.named_scope(name + "_" + "_".join(str(v) for v in args)):
            table[name](*args)

    with jax.named_scope("total"):
        arrived(sf.at[pl.ds(1, n - 1)], s_recv.at[1])
        sums = sf[0]
        for i in range(1, n):
            sums = sums + sf[i]
        total = jnp.sum(jnp.sum(sums, axis=0, keepdims=True), axis=1, keepdims=True)
        scale = lax.rsqrt(total / (3 * rank * width * tp) + SQUARE_EPS)

    outs = (c0_ref, c1_ref, c2_ref)
    chunks = [(m, h) for m in range(3) for h in range(2)]
    others_first = [(m, j, e) for e in range(nx) for j in range(nz) if j or e for m in range(3)]

    def chunk_span(m, h):
        first, rest = spans[m]
        cut = rest * CUTS[m] // 28 // 16 * 16
        return (first + cut, rest - cut) if h else (first, cut)

    def place(m, start, size, slot):
        if m < 2:
            return outs[m].at[pl.ds(pl.multiple_of(slot * block + start, 16), size), :]
        return outs[m].at[pl.ds(start, size), pl.ds(pl.multiple_of(slot * block, block), block)]

    def settle(m, start, size):
        r = pl.ds(start, size)
        update = scale * news[m][r, :]
        news[m][r, :] = update
        place(m, start, size, me)[...] = (wts[m][r, :] - LEARN_RATE * update).astype(BF16)

    def complete(m, j, e):
        slot = slot_of(j, e)
        first = spans[m][0]
        if e:
            arrived(early[m].at[slot], e_recv.at[m, slot])
        if m < 2:
            rows_in = fg[m, slot, pl.ds(0, first), :]
            update = jnp.dot(rows_in, dh[m], preferred_element_type=F32)
            update = update + jnp.dot(rows_in, dl[m], preferred_element_type=F32)
        else:
            cols = pl.ds(0, first)
            update = lax.dot_general(dh[2, :, cols], fg[2, slot], tdims, preferred_element_type=F32)
            update = update + lax.dot_general(dl[2, :, cols], fg[2, slot], tdims, preferred_element_type=F32)
        weight = decode(early[m][slot], WEIGHT_GAIN)
        place(m, 0, first, slot)[...] = (weight - LEARN_RATE * (scale * update)).astype(BF16)

    def forward(item, z_first, src, ssem, rsem):
        d, e, s1, s2, slot, valid = item
        n1, n2 = (nz, nx) if z_first else (nx, nz)
        c1, c2 = (z, x) if z_first else (x, z)
        st1, st2 = (nx, 1) if z_first else (1, nx)
        if e == 0 and d < n1 - 1:
            if s1 in (-1, 0):
                send(src, ssem, rsem, {"fs": me + st1}, c1 + 1 < n1, valid)
            if s1 in (1, 0):
                send(src, ssem, rsem, {"fs": me - st1}, c1 > 0, valid)
        if e < n2 - 1:
            if s2 in (-1, 0):
                send(src, ssem, rsem, {"fs": me + st2}, c2 + 1 < n2, valid)
            if s2 in (1, 0):
                send(src, ssem, rsem, {"fs": me - st2}, c2 > 0, valid)

    stages = nz + nx - 1
    last_waits = []
    each = -(-len(others_first) // (len(chunks) * (stages - FINISH - 1)))
    for s in range(stages):
        for c in range(6) if s == 0 else ORDER:
            m, h = chunks[c]
            z_first = c > 0
            start, size = chunk_span(m, h)
            if s == 0:
                settle(m, start, size)
            with jax.named_scope(f"gather_{s}_{c}"):
                for item in stage_items(s, z_first, nz, nx, z, x):
                    slot, valid = item[4], item[5]
                    dst = place(m, start, size, slot)
                    if item[1] == (nx if z_first else nz) - 1:
                        last_waits.append((dst, c_recv.at[c, slot], valid))
                        continue
                    if s > 0:
                        arrived(dst, c_recv.at[c, slot], valid)
                    forward(item, z_first, dst, c_send.at[c], c_recv.at[c, slot])
            if FINISH <= s < stages - 1:
                with jax.named_scope(f"complete_{s}_{c}"):
                    for task in others_first[:each]:
                        complete(*task)
                    others_first = others_first[each:]
        if s == 0:
            with jax.named_scope("late_early"):
                for late in range(3):
                    for d in range(len(EARLY_HOP[late]) + 1, nz):
                        e_hop(late, d)
                    if EARLY_X[late] is None:
                        e_cross(late)
                for m in range(3):
                    settle(m, 0, spans[m][0])
    with jax.named_scope("last_waits"):
        for dst, sem, valid in last_waits:
            arrived(dst, sem, valid)
    with jax.named_scope("drain"):
        for c, (m, h) in enumerate(chunks):
            counts = {}
            for cz in range(nz):
                for cx in range(nx):
                    counts.setdefault(gather_sends(nz, nx, cz, cx, c > 0), []).append(cz * nx + cx)
            for count, places in counts.items():
                here = functools.reduce(jnp.logical_or, [me == at for at in places])
                size = chunk_span(m, h)[1]
                size = size if m < 2 else size * block // width
                arrived(outs[0].at[pl.ds(0, count * size), :], c_send.at[c], here)
        last = pl.ds(0, n - 1)
        if relayed:
            arrived(fg.at[:, pl.ds(0, n - 2), pl.ds(0, FS_SHARE * unit), :], out_sem.at[F_OUT], outer)
            arrived(fg.at[:, pl.ds(0, n), pl.ds(0, FS_SHARE * unit), :], out_sem.at[F_OUT], inner)
        else:
            arrived(fg.at[:, last, pl.ds(0, FS_SHARE * unit), :], out_sem.at[F_OUT])
        arrived(fg.at[:, last, pl.ds(0, (8 - FS_SHARE) * unit), :], out_sem.at[Y_OUT])
        arrived(fg.at[:, last, pl.ds(0, block // 2), :], out_sem.at[P_OUT])
        arrived(xf.at[:, :, mine, :], out_sem.at[XF_OUT])
        arrived(part.at[:, pl.ds(0, nz * (nx - 1))], out_sem.at[RX_OUT])
        arrived(rz, out_sem.at[RZ_OUT])
        arrived(dg.at[:, last], out_sem.at[D_OUT])
        arrived(st.at[pl.ds(1, tp - 1)], out_sem.at[ST_OUT])
        arrived(sf.at[pl.ds(1, n - 1)], out_sem.at[SF_OUT])
        for m in range(3):
            size = spans[m][0] if m < 2 else spans[m][0] * block // width
            counts = {}
            for cz in range(nz):
                count = nz * (nx - 1) + (cz < nz - 1) * (cz + 1) + (cz > 0) * (nz - cz)
                counts.setdefault(count, []).append(cz)
            for count, places in counts.items():
                here = functools.reduce(jnp.logical_or, [z == at for at in places])
                arrived(outs[0].at[pl.ds(0, count * size), :], e_send.at[m], here)


def store_kernel(*refs):
    count = (len(refs) - 1) // 2
    sems = refs[-1]
    copies = [pltpu.make_async_copy(refs[i], refs[count + i], sems.at[i]) for i in range(count)]
    for copy in copies:
        copy.start()
    for copy in copies:
        copy.wait()


def shards(nz, nx, tp, *args):
    inputs, value_cot, gate_cot, out_cot, conv_output, factors, vw, gw, ow, m1, m2 = args
    n = nz * nx
    block, rank = factors.shape[1], factors.shape[2]
    rows, width = m1.shape[1], m1.shape[2]
    tokens = inputs.shape[0]
    features = inputs.shape[1]
    any_ = pl.BlockSpec(memory_space=pl.ANY)
    vmem = pl.BlockSpec(memory_space=pltpu.VMEM)
    dma = pltpu.SemaphoreType.DMA
    own = tokens // 2
    scratch = [
        pltpu.VMEM((own, features), BF16),
        pltpu.VMEM((own, features), BF16),
        pltpu.VMEM((3, tokens, width), BF16),
        pltpu.VMEM((3, n, block, rank), BF16),
        (pltpu.VMEM(vw.shape, F32), pltpu.VMEM(gw.shape, F32), pltpu.VMEM(ow.shape, F32)),
        pltpu.VMEM((3, own, rank), F32),
        pltpu.VMEM((3, 2, tokens, rank), BF16),
        pltpu.VMEM((3, n, rows, width), F32),
        pltpu.VMEM((3, nx - 1, nz, rows, width), F32),
        pltpu.VMEM((3, nz - 1, rows, width), F32),
        pltpu.VMEM((3, nz, rows, width), F32),
        pltpu.VMEM((3, n, rows, width), BF16),
        pltpu.VMEM((3, rank, width), BF16),
        pltpu.VMEM((3, rank, width), BF16),
        pltpu.VMEM((tp, 8, 128), F32),
        pltpu.VMEM((n, 8, 128), F32),
        (
            pltpu.VMEM((n, block * EARLY // EARLY_OF, width), BF16),
            pltpu.VMEM((n, block * EARLY // EARLY_OF, width), BF16),
            pltpu.VMEM((n, width * EARLY // EARLY_OF, block), BF16),
        ),
        dma((9,)),
        dma((3, n)), dma((3, n)), dma((3, n)), dma((3,)),
        dma((3, nx - 1, nz)), dma((3, nz - 1)), dma((3, n)), dma((2,)), dma((6, n)),
        dma((9,)), dma((6,)), dma((3, n)), dma((3,)),
    ]
    shape = [
        (m1.shape, F32), (m2.shape, F32), (vw.shape, F32), (gw.shape, F32), (ow.shape, F32),
        ((features, width), BF16), ((features, width), BF16), ((width, features), BF16),
    ]
    held = pl.pallas_call(
        functools.partial(kernel, nz, nx, tp, schedule(nz, nx)),
        out_shape=tuple(pltpu.VMEM(*item) for item in shape),
        in_specs=[any_] * 9 + [vmem] * 2,
        out_specs=(vmem,) * 8,
        scratch_shapes=scratch,
        compiler_params=pltpu.CompilerParams(
            collective_id=0, has_side_effects=True, vmem_limit_bytes=VMEM_BYTES
        ),
    )(inputs, out_cot, value_cot, gate_cot, conv_output, factors, vw, gw, ow, m1, m2)
    return pl.pallas_call(
        store_kernel,
        out_shape=tuple(jax.ShapeDtypeStruct(*item) for item in shape),
        in_specs=[vmem] * 8,
        out_specs=(any_,) * 8,
        scratch_shapes=[dma((8,))],
        compiler_params=pltpu.CompilerParams(vmem_limit_bytes=1024 * 1024),
    )(*held)


def solution(mesh):
    fs, tp = mesh.shape["fs"], mesh.shape["tp"]
    nz = 1 << (fs.bit_length() // 2)
    nx = fs // nz
    placed = (
        P("fs", None),
        P("fs", "tp"),
        P("fs", "tp"),
        P("fs", None),
        P("fs", "tp"),
        P(None, "fs", None),
        P("fs", "tp"),
        P("fs", "tp"),
        P("tp", "fs"),
        P(None, "fs", "tp"),
        P(None, "fs", "tp"),
    )
    return jax.shard_map(
        functools.partial(shards, nz, nx, tp),
        mesh=mesh,
        in_specs=placed,
        out_specs=(
            P(None, "fs", "tp"),
            P(None, "fs", "tp"),
            P("fs", "tp"),
            P("fs", "tp"),
            P("tp", "fs"),
            P(None, "tp"),
            P(None, "tp"),
            P("tp", None),
        ),
        check_vma=False,
    )
```

```python
import functools

import jax
import jax.numpy as jnp
from jax import lax
from jax.experimental import pallas as pl
from jax.experimental.pallas import tpu as pltpu
from jax.sharding import PartitionSpec as P

FIRST_DECAY = 0.9
SECOND_DECAY = 0.95
DIVISOR_EPS = 1e-08
SQUARE_EPS = 1e-06
LEARN_RATE = 0.01
K_STEP = 7.0
USE_LAG = 5.5
DIRECTION_GAIN = 128.0
WEIGHT_GAIN = 65536.0
EARLY = 3
EARLY_OF = 16
CUTS = (18, 14, 14)
PARTIAL = (24.0, 28.0, 36.0)
ALONG_Z = (28.6, 36.5, 42.5)
ALONG_STEP = (1.0, 0.3, 1.0)
MOMENTS = (38.0, 47.5, 51.0)
EARLY_Z = (16.0, 20.0, 51.05)
EARLY_HOP = ((21.5, 25.8, 30.0), (25.9, 30.1, 38.6), (55.3, 58.75))
EARLY_X = (39.0, 56.0, None)
OWN_X = (8.5, 12.5, 16.5)
FS_SHARE = 5
CODE_AT = 8.4
CROSS_LAG = 5.0
FINISH = 3
ORDER = (1, 2, 3, 4, 5, 0)
GATHER_D = (48.0, 51.1, 54.5)
LAST_D = (52.0, 55.5, 57.5)
VMEM_BYTES = 45 * 1024 * 1024
MESH = pl.DeviceIdType.MESH
F32 = jnp.float32
BF16 = jnp.bfloat16


def high_low(values):
    upper = values.astype(BF16)
    lower = (values - upper.astype(F32)).astype(BF16)
    return upper, lower


def others(coord, size, dist):
    if dist == 0:
        return [(coord, 0, None)]
    if size == 2:
        return [(1 - coord, None, None)]
    return [(coord - dist, -1, coord >= dist), (coord + dist, 1, coord + dist < size)]


def both(*preds):
    preds = [p for p in preds if p is not None]
    if not preds:
        return None
    return functools.reduce(jnp.logical_and, preds)


def run_if(pred, fn):
    if pred is None:
        fn()
    else:
        pl.when(pred)(fn)


def power(values):
    cube = values * values * values
    return cube * cube * cube


def encode(values, gain):
    return power(values * gain).astype(BF16)


def decode(coded, gain):
    value = coded.astype(F32)
    size = jnp.exp(jnp.log(jnp.abs(value)) * (1.0 / 9.0)) * (1.0 / gain)
    return jnp.where(value < 0.0, -size, size)


def stage_items(s, z_first, nz, nx, z, x):
    n1, n2 = (nz, nx) if z_first else (nx, nz)
    c1, c2 = (z, x) if z_first else (x, z)
    items = []
    for e in range(0, n2):
        d = s - e
        if d < 0 or d >= n1:
            continue
        for o1, s1, v1 in others(c1, n1, d):
            for o2, s2, v2 in others(c2, n2, e):
                slot = o1 * nx + o2 if z_first else o2 * nx + o1
                items.append((d, e, s1, s2, slot, both(v1, v2)))
    return items


def gather_sends(nz, nx, z, x, z_first):
    n1, n2 = (nz, nx) if z_first else (nx, nz)
    c1, c2 = (z, x) if z_first else (x, z)
    count = 0
    for o1 in range(n1):
        for o2 in range(n2):
            if o2 == c2:
                count += (o1 <= c1 < n1 - 1) + (o1 >= c1 > 0)
            count += (o2 <= c2 < n2 - 1) + (o2 >= c2 > 0)
    return count


def schedule(nz, nx):
    steps = []

    def add(at, name, *args):
        steps.append((at, name, args))

    def pieces(name, k, first, apart, behind, last):
        for e in range(nx):
            for j in range(nz):
                if j and not e:
                    add(first + apart * (j - 1), name, k, j, e)
                elif e:
                    add(behind if j == 0 else last + 0.4 * j, name, k, j, e)

    for k in range(3):
        at = K_STEP * k
        add(0.01 * k, "f_own_x", k)
        add(5.0 * k, "f_own_z", k)
        add(2.5 + at, "own_part", k)
        for e in range(nx):
            for j in range(nz):
                if j or e:
                    if j == 0:
                        there = 4.0 + 1.8 * k
                    else:
                        there = at + (5.0, 7.0, 9.0)[j - 1] + (CROSS_LAG if e else 0.0)
                    if j == nz - 1 and not e:
                        add(there - 1.9, "f_inner", k)
                        add(there, "f_outer", k)
                    else:
                        add(there, "f_arrive", k, j, e)
                    add(there + 3.2, "f_pass", k, j, e)
                    add(max(there + USE_LAG, at + 6.0), "f_use", k, j, e)
        add(at + 9.3 + CROSS_LAG + USE_LAG, "split", k)
        add(PARTIAL[k], "partial", k)
        for step, i in enumerate(list(range(1, nz)) + [0]):
            add(ALONG_Z[k] + ALONG_STEP[k] * step, "along_z", k, i)
        add(MOMENTS[k], "moments", k)
        pieces("d_arrive", k, GATHER_D[k], 0.3, GATHER_D[k] + 0.1, LAST_D[k])
        add(LAST_D[k] + 2.0, "unscaled", k)
    add(MOMENTS[2] + 1.5, "norm")
    for m in range(3):
        add(CODE_AT, "e_code", m)
        add(EARLY_Z[m], "e_own_z", m)
        add(OWN_X[m], "e_own_x", m)
        for d, hop_at in enumerate(EARLY_HOP[m]):
            add(hop_at, "e_hop", m, d + 1)
        if EARLY_X[m] is not None:
            add(EARLY_X[m], "e_cross", m)
    steps.sort(key=lambda step: step[0])
    return steps


def kernel(
    nz, nx, tp, steps_of,
    x_hbm, oc_hbm, vc_hbm, gc_hbm, co_hbm, f_hbm, w0_hbm, w1_hbm, w2_hbm, m1_ref, m2_ref,
    nf_ref, ns_ref, u0_ref, u1_ref, u2_ref, c0_ref, c1_ref, c2_ref,
    x_v, oc_v, cots, fg, wts, acc, xf, part, rx, rz, q, dg, dh, dl, st, sf, early,
    in_sem, f_recv, y_recv, p_recv, xf_recv, rx_recv, rz_recv, d_recv, s_recv, c_recv, out_sem, c_send, e_recv, e_send,
):
    me = lax.axis_index("fs")
    t = lax.axis_index("tp")
    z = lax.div(me, nx)
    x = lax.rem(me, nx)
    n = nz * nx
    core = lax.rem(t, 2)
    row = lax.rem(lax.div(t, 2), 2)
    mate = t + 1 - 2 * core
    beside = t + 2 - 4 * row
    block = f_hbm.shape[1]
    rank = f_hbm.shape[2]
    rows = m1_ref.shape[1]
    width = m1_ref.shape[2]
    own = x_v.shape[0]
    F_OUT, Y_OUT, P_OUT, XF_OUT, RX_OUT, RZ_OUT, D_OUT, ST_OUT, SF_OUT = range(9)

    def remote(src, dst, ssem, rsem, where):
        copy = pltpu.make_async_remote_copy(
            src_ref=src, dst_ref=dst, send_sem=ssem, recv_sem=rsem,
            device_id=where, device_id_type=MESH,
        )
        return copy

    def push(src, group, rsem, where, dst=None):
        remote(src, src if dst is None else dst, out_sem.at[group], rsem, where).start()

    def send(src, ssem, rsem, where, pred, outer):
        run_if(both(pred, outer), remote(src, src, ssem, rsem, where).start)

    def arrived(dst, sem, pred=None):
        run_if(pred, pltpu.make_async_copy(dst, dst, sem).wait)

    mine = pl.ds(pl.multiple_of(core * own, own), own)
    theirs = pl.ds(pl.multiple_of((1 - core) * own, own), own)
    loads = [
        pltpu.make_async_copy(f_hbm, fg.at[:, me], in_sem.at[0]),
        pltpu.make_async_copy(x_hbm.at[mine], x_v, in_sem.at[1]),
        pltpu.make_async_copy(oc_hbm.at[mine], oc_v, in_sem.at[2]),
        pltpu.make_async_copy(vc_hbm, cots.at[0], in_sem.at[3]),
        pltpu.make_async_copy(gc_hbm, cots.at[1], in_sem.at[4]),
        pltpu.make_async_copy(co_hbm, cots.at[2], in_sem.at[5]),
        pltpu.make_async_copy(w0_hbm, wts[0], in_sem.at[6]),
        pltpu.make_async_copy(w1_hbm, wts[1], in_sem.at[7]),
        pltpu.make_async_copy(w2_hbm, wts[2], in_sem.at[8]),
    ]
    for load in loads:
        load.start()

    barrier = pltpu.get_barrier_semaphore()
    everyone = [{"fs": lax.rem(me + k, n)} for k in range(1, n)]
    everyone += [{"tp": lax.rem(t + k, tp)} for k in range(1, tp)]
    for peer in everyone:
        pl.semaphore_signal(barrier, inc=1, device_id=peer, device_id_type=MESH)
    with jax.named_scope("barrier"):
        pl.semaphore_wait(barrier, len(everyone))

    def ranked(j):
        near = [sorted((abs(i - c), i) for i in range(nz))[j][1] for c in range(nz)]
        peer = near[0]
        for c in range(1, nz):
            peer = jnp.where(z == c, near[c], peer)
        return peer

    zs = [ranked(j) for j in range(nz)]
    xs = [lax.rem(x + e, nx) for e in range(nx)]

    def slot_of(j, e):
        return zs[j] * nx + xs[e] if j or e else me

    unit = block // 16
    half = core * (block // 2)
    fs_start = pl.multiple_of(half + row * (8 - FS_SHARE) * unit, unit)
    y_send_start = pl.multiple_of(half + row * FS_SHARE * unit, unit)
    y_recv_start = pl.multiple_of(half + (1 - row) * FS_SHARE * unit, unit)
    mate_half = pl.multiple_of((1 - core) * (block // 2), block // 2)

    def f_part(k, slot, start, size):
        return fg.at[k, slot, pl.ds(start, size), :]

    sources = (x_v, x_v, oc_v)
    spans = [(wide * EARLY // EARLY_OF, wide - wide * EARLY // EARLY_OF) for wide in (block, block, width)]

    def e_push(m, slot, where, index):
        piece = early[m].at[slot]
        remote(piece, piece, e_send.at[m], e_recv.at[m, index], {"fs": where}).start()

    def e_code(m):
        loads[6 + m].wait()
        early[m][me] = encode(wts[m][pl.ds(0, spans[m][0]), :], WEIGHT_GAIN)

    def e_own_z(m):
        run_if(z < nz - 1, lambda: e_push(m, me, me + nx, z))
        run_if(z > 0, lambda: e_push(m, me, me - nx, z))

    def e_hop(m, d):
        for up, peer in ((1, z - d), (-1, z + d)):
            slot = peer * nx + x

            def relay(up=up, slot=slot, peer=peer):
                arrived(early[m].at[slot], e_recv.at[m, peer])
                onward = z + up
                run_if(jnp.logical_and(onward >= 0, onward < nz), lambda: e_push(m, slot, me + up * nx, peer))

            run_if(jnp.logical_and(peer >= 0, peer < nz), relay)

    def e_own_x(m):
        for e in range(1, nx):
            e_push(m, me, slot_of(0, e), z)

    def e_cross(m):
        for j in range(1, nz):
            for e in range(1, nx):
                e_push(m, slot_of(j, 0), slot_of(0, e), z)

    def matmul(k, slot, first):
        cols = pl.ds(pl.multiple_of(slot * block, block), block)
        tile = 256

        def body(i, carry):
            r = pl.ds(pl.multiple_of(i * tile, tile), tile)
            prod = jnp.dot(sources[k][r, cols], fg[k, slot], preferred_element_type=F32)
            if first:
                acc[k, r, :] = prod
            else:
                acc[k, r, :] += prod
            return carry

        lax.fori_loop(0, own // tile, body, 0)

    relayed = nz == 4
    inner = jnp.logical_and(z > 0, z < nz - 1)
    outer = jnp.logical_not(inner)

    def f_own_z(k):
        piece = f_part(k, me, fs_start, FS_SHARE * unit)
        for j in range(1, nz):
            copy = remote(piece, piece, out_sem.at[F_OUT], f_recv.at[k, me], {"fs": slot_of(j, 0)})
            run_if(inner if relayed and j == nz - 1 else None, copy.start)

    def f_inner(k):
        def relay():
            f_arrive(k, nz - 1, 0)
            slot = slot_of(nz - 1, 0)
            end = (z - 1) * (nz - 1)
            push(f_part(k, slot, fs_start, FS_SHARE * unit), F_OUT, f_recv.at[k, slot], {"fs": end * nx + x})

        if relayed:
            run_if(inner, relay)

    def f_outer(k):
        run_if(outer if relayed else None, lambda: f_arrive(k, nz - 1, 0))

    def f_own_x(k):
        piece = f_part(k, me, fs_start, FS_SHARE * unit)
        for e in range(1, nx):
            push(piece, F_OUT, f_recv.at[k, me], {"fs": slot_of(0, e)})

    def f_arrive(k, j, e):
        slot = slot_of(j, e)
        piece = f_part(k, slot, fs_start, FS_SHARE * unit)
        arrived(piece, f_recv.at[k, slot])
        if e == 0:
            for other in range(1, nx):
                push(piece, F_OUT, f_recv.at[k, slot], {"fs": slot_of(0, other)})
        push(f_part(k, slot, y_send_start, (8 - FS_SHARE) * unit), Y_OUT, y_recv.at[k, slot], {"tp": beside})
        push(piece, P_OUT, p_recv.at[k, slot], {"tp": mate})

    def f_pass(k, j, e):
        slot = slot_of(j, e)
        piece = f_part(k, slot, y_recv_start, (8 - FS_SHARE) * unit)
        arrived(piece, y_recv.at[k, slot])
        push(piece, P_OUT, p_recv.at[k, slot], {"tp": mate})

    def f_use(k, j, e):
        slot = slot_of(j, e)
        arrived(f_part(k, slot, mate_half, block // 2), p_recv.at[k, slot])
        matmul(k, slot, False)

    def own_part(k):
        if k != 1:
            loads[1 + k // 2].wait()
        matmul(k, me, True)

    dims = (((0,), (0,)), ((), ()))

    def product(k, r):
        prod = lax.dot_general(xf[k, 0, r, :], cots[k, r, :], dims, preferred_element_type=F32)
        prod = prod + lax.dot_general(xf[k, 1, r, :], cots[k, r, :], dims, preferred_element_type=F32)
        return prod.reshape(n, rows, width)

    def split(k):
        upper, lower = high_low(acc[k])
        xf[k, 0, mine, :] = upper
        xf[k, 1, mine, :] = lower
        push(xf.at[k, :, mine, :], XF_OUT, xf_recv.at[k], {"tp": mate})
        loads[3 + k].wait()
        part[k] = product(k, mine)

    order = list(range(1, nz)) + [0]

    def partial(k):
        arrived(xf.at[k, :, theirs, :], xf_recv.at[k])
        part[k] = part[k] + product(k, theirs)
        for i in order:
            oz = lax.rem(z + i, nz)
            for e in range(1, nx):
                slot = oz * nx + xs[e]
                push(part.at[k, slot], RX_OUT, rx_recv.at[k, e - 1, i], {"fs": z * nx + xs[e]}, rx.at[k, e - 1, i])

    def along_z(k, i):
        oz = lax.rem(z + i, nz)
        value = part[k, oz * nx + x]
        for e in range(1, nx):
            arrived(rx.at[k, e - 1, i], rx_recv.at[k, e - 1, i])
            value = value + rx[k, e - 1, i]
        q[k, i] = value
        if i:
            push(q.at[k, i], RZ_OUT, rz_recv.at[k], {"fs": oz * nx + x}, rz.at[k, i - 1])

    def moments(k):
        projected = q[k, 0]
        arrived(rz.at[k], rz_recv.at[k])
        for i in range(1, nz):
            projected = projected + rz[k, i - 1]
        new_first = FIRST_DECAY * m1_ref[k] + (1.0 - FIRST_DECAY) * projected
        new_second = SECOND_DECAY * m2_ref[k] + (1.0 - SECOND_DECAY) * projected * projected
        nf_ref[k] = new_first
        ns_ref[k] = new_second
        direction = new_first / (jnp.sqrt(new_second) + DIVISOR_EPS)
        dg[k, me] = encode(direction, DIRECTION_GAIN)
        piece = dg.at[k, me]
        for j in range(nz - 1, 0, -1):
            push(piece, D_OUT, d_recv.at[k, z], {"fs": slot_of(j, 0)})
        for e in range(1, nx):
            push(piece, D_OUT, d_recv.at[k, z], {"fs": slot_of(0, e)})
        square = jnp.sum((direction * direction).reshape(rows * width // 1024, 8, 128), axis=0)
        st[0] = square if k == 0 else st[0] + square
        if k == 2:
            for i in range(1, tp):
                push(st.at[0], ST_OUT, s_recv.at[0], {"tp": lax.rem(t + i, tp)}, st.at[tp - i])

    def norm():
        arrived(st.at[pl.ds(1, tp - 1)], s_recv.at[0])
        value = st[0]
        for i in range(1, tp):
            value = value + st[i]
        sf[0] = value
        for i in range(1, n):
            push(sf.at[0], SF_OUT, s_recv.at[1], {"fs": lax.rem(me + i, n)}, sf.at[n - i])

    def d_arrive(k, j, e):
        slot = slot_of(j, e)
        piece = dg.at[k, slot]
        if e == 0:
            arrived(piece, d_recv.at[k, zs[j]])
            for other in range(1, nx):
                push(piece, D_OUT, d_recv.at[k, z], {"fs": slot_of(0, other)})
        elif e == nx - 1 and j == nz - 1:
            arrived(dg.at[k, pl.ds(0, nz * (nx - 1))], d_recv.at[k, z])

    tdims = (((0,), (1,)), ((), ()))
    news = (u0_ref, u1_ref, u2_ref)

    def unscaled(k):
        value = decode(dg[k].reshape(rank, width), DIRECTION_GAIN)
        upper, lower = high_low(value)
        dh[k] = upper
        dl[k] = lower
        if k < 2:
            news[k][...] = jnp.dot(fg[k, me], dh[k], preferred_element_type=F32) + jnp.dot(
                fg[k, me], dl[k], preferred_element_type=F32
            )
        else:
            news[k][...] = lax.dot_general(dh[k], fg[k, me], tdims, preferred_element_type=F32) + lax.dot_general(
                dl[k], fg[k, me], tdims, preferred_element_type=F32
            )

    table = dict(
        f_own_z=f_own_z, f_own_x=f_own_x, f_arrive=f_arrive, f_pass=f_pass, f_use=f_use, own_part=own_part,
        split=split, partial=partial, along_z=along_z, moments=moments, d_arrive=d_arrive, norm=norm,
        unscaled=unscaled, e_code=e_code, e_own_z=e_own_z, e_own_x=e_own_x, e_hop=e_hop, e_cross=e_cross, f_inner=f_inner, f_outer=f_outer,
    )
    loads[0].wait()
    for _, name, args in steps_of:
        with jax.named_scope(name + "_" + "_".join(str(v) for v in args)):
            table[name](*args)

    with jax.named_scope("total"):
        arrived(sf.at[pl.ds(1, n - 1)], s_recv.at[1])
        sums = sf[0]
        for i in range(1, n):
            sums = sums + sf[i]
        total = jnp.sum(jnp.sum(sums, axis=0, keepdims=True), axis=1, keepdims=True)
        scale = lax.rsqrt(total / (3 * rank * width * tp) + SQUARE_EPS)

    outs = (c0_ref, c1_ref, c2_ref)
    chunks = [(m, h) for m in range(3) for h in range(2)]
    others_first = [(m, j, e) for e in range(nx) for j in range(nz) if j or e for m in range(3)]

    def chunk_span(m, h):
        first, rest = spans[m]
        cut = rest * CUTS[m] // 28 // 16 * 16
        return (first + cut, rest - cut) if h else (first, cut)

    def place(m, start, size, slot):
        if m < 2:
            return outs[m].at[pl.ds(pl.multiple_of(slot * block + start, 16), size), :]
        return outs[m].at[pl.ds(start, size), pl.ds(pl.multiple_of(slot * block, block), block)]

    def settle(m, start, size):
        r = pl.ds(start, size)
        update = scale * news[m][r, :]
        news[m][r, :] = update
        place(m, start, size, me)[...] = (wts[m][r, :] - LEARN_RATE * update).astype(BF16)

    def complete(m, j, e):
        slot = slot_of(j, e)
        first = spans[m][0]
        if e == 1 and j == 0:
            arrived(early[m].at[pl.ds(0, nz * (nx - 1))], e_recv.at[m, z])
        if m < 2:
            rows_in = fg[m, slot, pl.ds(0, first), :]
            update = jnp.dot(rows_in, dh[m], preferred_element_type=F32)
            update = update + jnp.dot(rows_in, dl[m], preferred_element_type=F32)
        else:
            cols = pl.ds(0, first)
            update = lax.dot_general(dh[2, :, cols], fg[2, slot], tdims, preferred_element_type=F32)
            update = update + lax.dot_general(dl[2, :, cols], fg[2, slot], tdims, preferred_element_type=F32)
        weight = decode(early[m][slot], WEIGHT_GAIN)
        place(m, 0, first, slot)[...] = (weight - LEARN_RATE * (scale * update)).astype(BF16)

    def forward(item, z_first, src, ssem, rsem):
        d, e, s1, s2, slot, valid = item
        n1, n2 = (nz, nx) if z_first else (nx, nz)
        c1, c2 = (z, x) if z_first else (x, z)
        st1, st2 = (nx, 1) if z_first else (1, nx)
        if e == 0 and d < n1 - 1:
            if s1 in (-1, 0):
                send(src, ssem, rsem, {"fs": me + st1}, c1 + 1 < n1, valid)
            if s1 in (1, 0):
                send(src, ssem, rsem, {"fs": me - st1}, c1 > 0, valid)
        if e < n2 - 1:
            if s2 in (-1, 0):
                send(src, ssem, rsem, {"fs": me + st2}, c2 + 1 < n2, valid)
            if s2 in (1, 0):
                send(src, ssem, rsem, {"fs": me - st2}, c2 > 0, valid)

    stages = nz + nx - 1
    last_waits = []
    each = -(-len(others_first) // (len(chunks) * (stages - FINISH - 1)))
    for s in range(stages):
        for c in range(6) if s == 0 else ORDER:
            m, h = chunks[c]
            z_first = c > 0
            start, size = chunk_span(m, h)
            if s == 0:
                settle(m, start, size)
            with jax.named_scope(f"gather_{s}_{c}"):
                for item in stage_items(s, z_first, nz, nx, z, x):
                    slot, valid = item[4], item[5]
                    dst = place(m, start, size, slot)
                    if item[1] == (nx if z_first else nz) - 1:
                        last_waits.append((dst, c_recv.at[c, slot], valid))
                        continue
                    if s > 0:
                        arrived(dst, c_recv.at[c, slot], valid)
                    forward(item, z_first, dst, c_send.at[c], c_recv.at[c, slot])
            if FINISH <= s < stages - 1:
                with jax.named_scope(f"complete_{s}_{c}"):
                    for task in others_first[:each]:
                        complete(*task)
                    others_first = others_first[each:]
        if s == 0:
            with jax.named_scope("late_early"):
                for late in range(3):
                    for d in range(len(EARLY_HOP[late]) + 1, nz):
                        e_hop(late, d)
                    if EARLY_X[late] is None:
                        e_cross(late)
                for m in range(3):
                    settle(m, 0, spans[m][0])
    with jax.named_scope("last_waits"):
        for dst, sem, valid in last_waits:
            arrived(dst, sem, valid)
    with jax.named_scope("drain"):
        for c, (m, h) in enumerate(chunks):
            counts = {}
            for cz in range(nz):
                for cx in range(nx):
                    counts.setdefault(gather_sends(nz, nx, cz, cx, c > 0), []).append(cz * nx + cx)
            for count, places in counts.items():
                here = functools.reduce(jnp.logical_or, [me == at for at in places])
                size = chunk_span(m, h)[1]
                size = size if m < 2 else size * block // width
                arrived(outs[0].at[pl.ds(0, count * size), :], c_send.at[c], here)
        last = pl.ds(0, n - 1)
        if relayed:
            arrived(fg.at[:, pl.ds(0, n - 2), pl.ds(0, FS_SHARE * unit), :], out_sem.at[F_OUT], outer)
            arrived(fg.at[:, pl.ds(0, n), pl.ds(0, FS_SHARE * unit), :], out_sem.at[F_OUT], inner)
        else:
            arrived(fg.at[:, last, pl.ds(0, FS_SHARE * unit), :], out_sem.at[F_OUT])
        arrived(fg.at[:, last, pl.ds(0, (8 - FS_SHARE) * unit), :], out_sem.at[Y_OUT])
        arrived(fg.at[:, last, pl.ds(0, block // 2), :], out_sem.at[P_OUT])
        arrived(xf.at[:, :, mine, :], out_sem.at[XF_OUT])
        arrived(part.at[:, pl.ds(0, nz * (nx - 1))], out_sem.at[RX_OUT])
        arrived(rz, out_sem.at[RZ_OUT])
        arrived(dg.at[:, last], out_sem.at[D_OUT])
        arrived(st.at[pl.ds(1, tp - 1)], out_sem.at[ST_OUT])
        arrived(sf.at[pl.ds(1, n - 1)], out_sem.at[SF_OUT])
        for m in range(3):
            size = spans[m][0] if m < 2 else spans[m][0] * block // width
            counts = {}
            for cz in range(nz):
                count = nz * (nx - 1) + (cz < nz - 1) * (cz + 1) + (cz > 0) * (nz - cz)
                counts.setdefault(count, []).append(cz)
            for count, places in counts.items():
                here = functools.reduce(jnp.logical_or, [z == at for at in places])
                arrived(outs[0].at[pl.ds(0, count * size), :], e_send.at[m], here)


def store_kernel(*refs):
    count = (len(refs) - 1) // 2
    sems = refs[-1]
    copies = [pltpu.make_async_copy(refs[i], refs[count + i], sems.at[i]) for i in range(count)]
    for copy in copies:
        copy.start()
    for copy in copies:
        copy.wait()


def shards(nz, nx, tp, *args):
    inputs, value_cot, gate_cot, out_cot, conv_output, factors, vw, gw, ow, m1, m2 = args
    n = nz * nx
    block, rank = factors.shape[1], factors.shape[2]
    rows, width = m1.shape[1], m1.shape[2]
    tokens = inputs.shape[0]
    features = inputs.shape[1]
    any_ = pl.BlockSpec(memory_space=pl.ANY)
    vmem = pl.BlockSpec(memory_space=pltpu.VMEM)
    dma = pltpu.SemaphoreType.DMA
    own = tokens // 2
    scratch = [
        pltpu.VMEM((own, features), BF16),
        pltpu.VMEM((own, features), BF16),
        pltpu.VMEM((3, tokens, width), BF16),
        pltpu.VMEM((3, n, block, rank), BF16),
        (pltpu.VMEM(vw.shape, F32), pltpu.VMEM(gw.shape, F32), pltpu.VMEM(ow.shape, F32)),
        pltpu.VMEM((3, own, rank), F32),
        pltpu.VMEM((3, 2, tokens, rank), BF16),
        pltpu.VMEM((3, n, rows, width), F32),
        pltpu.VMEM((3, nx - 1, nz, rows, width), F32),
        pltpu.VMEM((3, nz - 1, rows, width), F32),
        pltpu.VMEM((3, nz, rows, width), F32),
        pltpu.VMEM((3, n, rows, width), BF16),
        pltpu.VMEM((3, rank, width), BF16),
        pltpu.VMEM((3, rank, width), BF16),
        pltpu.VMEM((tp, 8, 128), F32),
        pltpu.VMEM((n, 8, 128), F32),
        (
            pltpu.VMEM((n, block * EARLY // EARLY_OF, width), BF16),
            pltpu.VMEM((n, block * EARLY // EARLY_OF, width), BF16),
            pltpu.VMEM((n, width * EARLY // EARLY_OF, block), BF16),
        ),
        dma((9,)),
        dma((3, n)), dma((3, n)), dma((3, n)), dma((3,)),
        dma((3, nx - 1, nz)), dma((3,)), dma((3, nz)), dma((2,)), dma((6, n)),
        dma((9,)), dma((6,)), dma((3, nz)), dma((3,)),
    ]
    shape = [
        (m1.shape, F32), (m2.shape, F32), (vw.shape, F32), (gw.shape, F32), (ow.shape, F32),
        ((features, width), BF16), ((features, width), BF16), ((width, features), BF16),
    ]
    held = pl.pallas_call(
        functools.partial(kernel, nz, nx, tp, schedule(nz, nx)),
        out_shape=tuple(pltpu.VMEM(*item) for item in shape),
        in_specs=[any_] * 9 + [vmem] * 2,
        out_specs=(vmem,) * 8,
        scratch_shapes=scratch,
        compiler_params=pltpu.CompilerParams(
            collective_id=0, has_side_effects=True, vmem_limit_bytes=VMEM_BYTES
        ),
    )(inputs, out_cot, value_cot, gate_cot, conv_output, factors, vw, gw, ow, m1, m2)
    return pl.pallas_call(
        store_kernel,
        out_shape=tuple(jax.ShapeDtypeStruct(*item) for item in shape),
        in_specs=[vmem] * 8,
        out_specs=(any_,) * 8,
        scratch_shapes=[dma((8,))],
        compiler_params=pltpu.CompilerParams(vmem_limit_bytes=1024 * 1024),
    )(*held)


def solution(mesh):
    fs, tp = mesh.shape["fs"], mesh.shape["tp"]
    nz = 1 << (fs.bit_length() // 2)
    nx = fs // nz
    placed = (
        P("fs", None),
        P("fs", "tp"),
        P("fs", "tp"),
        P("fs", None),
        P("fs", "tp"),
        P(None, "fs", None),
        P("fs", "tp"),
        P("fs", "tp"),
        P("tp", "fs"),
        P(None, "fs", "tp"),
        P(None, "fs", "tp"),
    )
    return jax.shard_map(
        functools.partial(shards, nz, nx, tp),
        mesh=mesh,
        in_specs=placed,
        out_specs=(
            P(None, "fs", "tp"),
            P(None, "fs", "tp"),
            P("fs", "tp"),
            P("fs", "tp"),
            P("tp", "fs"),
            P(None, "tp"),
            P(None, "tp"),
            P("tp", None),
        ),
        check_vma=False,
    )
```
